32 devices in a mesh: ep: 4 (over y, x), tp: 8 (over z, core).
Axes of the slice: x: 2, y: 2, z: 4, core: 2. Of those that a mesh axis runs over, the one named last changes fastest.
Arguments:
- queries: bfloat16 [4096, 1024], P('ep', 'tp'), may hold values from -6 to 6
- keys: bfloat16 [4096, 256], P('ep'), may hold values from -6 to 6, as said below
- values: bfloat16 [4096, 256], P('ep'), may hold values from -6 to 6
- slopes: float32 [16], P('tp'), may hold values from 0.002 to 0.08
- sinks: float32 [16], P('tp'), may hold values from 2 to 6
- out_weight: bfloat16 [1024, 2048], P('tp'), may hold values from -0.1875 to 0.1875
- mix_gain: float32 [2048], replicated, may hold values from 0.1 to 1.9
- moe_input: bfloat16 [4096, 2048], P(('ep', 'tp')), may hold values from -6 to 6
- in_gain: float32 [2048], replicated, may hold values from 0.1 to 1.9
- out_gain: float32 [2048], replicated, may hold values from 0.1 to 1.9
- group_router: bfloat16 [2048, 4], replicated, may hold values from -0.125 to 0.125
- expert_router: bfloat16 [2048, 4], replicated, may hold values from -0.125 to 0.125
- routes: int32 [4096, 2], P(('ep', 'tp')), may hold values from 0 to 3, all different within a row; in each aligned block of 128 rows (0 to 127, 128 to 255, ...) at most 96 rows name the same one
- gate_weight: bfloat16 [4, 2048, 1024], P('ep', None, 'tp'), may hold values from -0.125 to 0.125
- up_weight: bfloat16 [4, 2048, 1024], P('ep', None, 'tp'), may hold values from -0.125 to 0.125
- down_weight: bfloat16 [4, 2048, 1024], P('ep', None, 'tp'), may hold values from -0.1875 to 0.1875
Outputs:
- mixer_output: bfloat16 [4096, 2048], P(('ep', 'tp'))
- moe_output: bfloat16 [4096, 2048], P(('ep', 'tp'))
The draws below stay inside these ranges and needn't reach their ends.
Inputs may be any that keep to these rules, and one draw needn't show every extreme that they name: `keys`: keys share one value range with the queries. `routes`: A token names 2 different experts. Among the rows of one device no expert is named more than 96 times, a bound that some block reaches in every draw.
All inputs are finite; a program needn't handle non-finite values.
Results may differ from the reference program's by a relative error of at most 0.018.
Values may be sent and summed in bfloat16 or wider, within the bound.
A program may use at most 128 MiB of HBM per device.

```python
import math
import jax
import jax.numpy as jnp
import numpy as np
from jax import lax

D = 2048
HEADS = 16
HD = 64
KV_HEADS = 4
WINDOW = 128
DE = 1024
GROUPS = 4
TOP = 2
TOK_DEV = 128
EXPERTS = 4
CAP = 96
TOKENS = 4096
N_TP = 8


def draw_keys(key, part):
    drawn = jnp.clip(jax.random.normal(jax.random.fold_in(key, 3), (TOKENS, KV_HEADS, HD), jnp.float32), -5.9, 5.9)
    return drawn.reshape(TOKENS, KV_HEADS * HD).astype(jnp.bfloat16)


def draw_queries(key, part):
    drawn = jnp.clip(jax.random.normal(jax.random.fold_in(key, 4), (TOKENS, HEADS, HD), jnp.float32), -5.9, 5.9)
    return drawn.reshape(TOKENS, HEADS * HD).astype(jnp.bfloat16)


def block_scale(rng, shape, shards, smallest, top_value):
    level = 1.0
    for dim, blocks in shards:
        heights = jax.random.uniform(jax.random.fold_in(jax.random.fold_in(rng, 6), dim), (blocks,), jnp.float32, smallest / len(shards), top_value / len(shards))
        level = level * jnp.repeat(jnp.exp(heights), shape[dim] // blocks).reshape((-1,) + (1,) * (len(shape) - 1 - dim))
    return level


def assign_block(key, own, number, rows, amount, top, reach, skew):
    sequence = jax.random.permutation(key, amount)
    heavy_load, common = portions_of(amount, rows * top, reach, skew, True), portions_of(amount, rows * top, reach, skew, False)
    places = jnp.arange(amount)

    def named(sizes, rotation):
        used = int((sizes > 0).sum())
        fixed = max(1, used // 4)
        passed = fixed + (places - fixed + rotation * (used - fixed)) % max(1, amount - fixed)
        return jnp.zeros((amount,), jnp.int32).at[sequence[jnp.where(places < fixed, places, passed)]].set(jnp.asarray(sizes, jnp.int32))

    sizes = jnp.where(number % 4 == 0, named(heavy_load, number // 4), named(common, number - number // 4 - 1))
    mixed = jax.random.permutation(jax.random.fold_in(own, 3), amount)
    giver, receiver = mixed[0:amount // 2 * 2:2], mixed[1:amount // 2 * 2:2]
    slack = jnp.minimum(sizes[giver] - 1, reach - sizes[receiver]) // 2
    slack = jnp.where((giver == sequence[0]) | (receiver == sequence[0]) | (sizes[receiver] == 0), 0, jnp.maximum(slack, 0))
    passed = jax.random.randint(jax.random.fold_in(own, 4), (amount // 2,), 0, 1 << 20) % (slack + 1)
    sizes = sizes.at[giver].add(-passed).at[receiver].add(passed)
    items = jnp.searchsorted(jnp.cumsum(sizes), jnp.arange(rows * top), side="right").astype(jnp.int32)
    listing = items.reshape(top, rows).T
    listing = listing[jax.random.permutation(jax.random.fold_in(own, 1), rows)]
    rotation = jax.random.randint(jax.random.fold_in(own, 2), (rows, 1), 0, top)
    return jnp.take_along_axis(listing, (jnp.arange(top)[None, :] + rotation) % top, axis=1)


def portions_of(count, total, reach, slope, full):
    loads = [(1 << 20) // math.isqrt(standing ** slope) + 1 for standing in range(1, count + 1)]
    largest = reach if full else min(reach, max(-(-total // count), total * loads[0] // sum(loads)))
    least = 1 if total - largest >= count - 1 else 0
    counts, rest = [largest] + [least] * (count - 1), total - largest - least * (count - 1)
    while rest > 0:
        free = [i for i in range(1, count) if counts[i] < largest] or [i for i in range(1, count) if counts[i] < reach]
        whole, left = sum([loads[i] for i in free]), rest
        for i in free:
            more = min(reach - counts[i], max(1, left * loads[i] // whole), rest)
            counts[i] = counts[i] + more
            rest = rest - more
    return np.array(counts)


def noise(stream_key, shape, spread, reach, pieces=(), kind=jnp.bfloat16):
    result = jax.random.normal(stream_key, shape, jnp.float32) * spread
    if len(pieces) > 0:
        result = block_scale(stream_key, shape, pieces, -0.22, 0.18) * result
    return jnp.clip(result, min=-reach, max=reach).astype(kind)


def setup_inputs(seed: int = 0) -> dict:
    arg_keys = jax.random.split(jax.random.key(seed), 17)
    queries = draw_queries(jax.random.fold_in(arg_keys[16], 71), 0)
    keys = draw_keys(jax.random.fold_in(arg_keys[16], 71), 0)
    values = noise(arg_keys[2], (TOKENS, KV_HEADS * HD), 1.0, 6.0, ((0, 4),))
    slopes = jnp.clip(jnp.exp(math.log(0.08) - 3.6888794 * jax.random.uniform(arg_keys[3], (HEADS,), jnp.float32) ** block_scale(arg_keys[3], (HEADS,), ((0, 8),), -0.2, 0.2)), 0.002, 0.08)
    sinks = jnp.clip(2.0 + 4.0 * jax.random.uniform(arg_keys[4], (HEADS,), jnp.float32) ** block_scale(arg_keys[4], (HEADS,), ((0, 8),), -0.2, 0.2), 2.0, 6.0)
    out_weight = noise(arg_keys[5], (HEADS * HD, D), (HEADS * HD) ** -0.5, 0.1875, ((0, 8),))
    mix_gain = jnp.clip(1.0 + 0.18 * jax.random.normal(arg_keys[6], (D,), jnp.float32), 0.1, 1.9)
    moe_input = noise(arg_keys[7], (TOKENS, D), 1.0, 6.0, ((0, 32),))
    in_gain = jnp.clip(1.0 + 0.18 * jax.random.normal(arg_keys[8], (D,), jnp.float32), 0.1, 1.9)
    out_gain = jnp.clip(1.0 + 0.18 * jax.random.normal(arg_keys[9], (D,), jnp.float32), 0.1, 1.9)
    group_router = noise(arg_keys[10], (D, GROUPS), D ** -0.5, 0.125)
    expert_router = noise(arg_keys[11], (D, EXPERTS), D ** -0.5, 0.125)
    routes_keys = jax.random.split(jax.random.fold_in(arg_keys[12], 1), TOKENS // TOK_DEV)
    routes_turns = jax.random.permutation(jax.random.fold_in(arg_keys[12], 3), TOKENS // TOK_DEV)
    routes = jax.vmap(lambda own, number: assign_block(jax.random.fold_in(arg_keys[12], 2), own, number, TOK_DEV, EXPERTS, TOP, CAP, 2))(routes_keys, routes_turns).reshape((TOKENS, TOP))
    gate_weight = noise(arg_keys[13], (EXPERTS, D, DE), D ** -0.5, 0.125, ((0, 4), (2, 8)))
    up_weight = noise(arg_keys[14], (EXPERTS, D, DE), D ** -0.5, 0.125, ((0, 4), (2, 8)))
    down_weight = noise(arg_keys[15], (EXPERTS, D, DE), DE ** -0.5, 0.1875, ((0, 4), (2, 8)))
    return dict(queries=queries, keys=keys, values=values, slopes=slopes, sinks=sinks, out_weight=out_weight, mix_gain=mix_gain, moe_input=moe_input, in_gain=in_gain, out_gain=out_gain, group_router=group_router, expert_router=expert_router, routes=routes, gate_weight=gate_weight, up_weight=up_weight, down_weight=down_weight)


eps = 1e-06

def scale_rows(matrix, gain):
    mean_square = lax.optimization_barrier(jnp.mean(matrix * matrix, axis=-1, keepdims=True))
    return matrix * lax.rsqrt(mean_square + eps) * gain

def attend(queries, keys, values, slopes, sinks):
    per_kv = HEADS // KV_HEADS
    blocks = TOKENS // WINDOW
    query_blocks = queries.astype(jnp.float32).reshape(blocks, WINDOW, KV_HEADS, per_kv, HD)
    key_blocks = keys.astype(jnp.float32).reshape(blocks, WINDOW, KV_HEADS, HD)
    value_blocks = values.astype(jnp.float32).reshape(blocks, WINDOW, KV_HEADS, HD)
    empty = jnp.zeros((1, WINDOW, KV_HEADS, HD), jnp.float32)
    key_span = jnp.concatenate([jnp.concatenate([empty, key_blocks[:-1]], axis=0), key_blocks], axis=1)
    value_span = jnp.concatenate([jnp.concatenate([empty, value_blocks[:-1]], axis=0), value_blocks], axis=1)
    scores = jnp.einsum('nqkgd,nskd->nkgqs', query_blocks, key_span) * (1.0 / math.sqrt(HD))
    query_index = jnp.arange(WINDOW, dtype=jnp.int32)[:, None]
    key_index = jnp.arange(2 * WINDOW, dtype=jnp.int32)[None, :]
    distance = query_index + WINDOW - key_index
    key_position = jnp.arange(blocks, dtype=jnp.int32)[:, None, None] * WINDOW + key_index[None] - WINDOW
    valid = ((distance >= 0) & (distance < WINDOW))[None] & (key_position >= 0)
    slope_table = slopes.reshape(KV_HEADS, per_kv)
    scores = scores - slope_table[None, :, :, None, None] * distance.astype(jnp.float32)[None, None, None]
    scores = jnp.where(valid[:, None, None], scores, -jnp.inf)
    sink = sinks.reshape(KV_HEADS, per_kv)[None, :, :, None, None]
    top = jnp.maximum(lax.optimization_barrier(jnp.max(scores, axis=-1, keepdims=True)), sink)
    weights = jnp.exp(scores - top)
    denom = lax.optimization_barrier(jnp.sum(weights, axis=-1, keepdims=True)) + jnp.exp(sink - top)
    probs = (weights / denom).astype(jnp.bfloat16)
    attention = jnp.einsum('nkgqs,nskd->nqkgd', probs.astype(jnp.float32), value_span)
    return attention.astype(jnp.bfloat16).reshape(TOKENS, HEADS * HD)

def reference(queries, keys, values, slopes, sinks, out_weight, mix_gain, moe_input, in_gain, out_gain, group_router, expert_router, routes, gate_weight, up_weight, down_weight):
    attention = attend(queries, keys, values, slopes, sinks)
    shard = HEADS * HD // N_TP
    projected = jnp.zeros((TOKENS, D), jnp.float32)
    for shard_index in range(N_TP):
        lower = shard_index * shard
        part = jnp.dot(attention[:, lower:lower + shard], out_weight[lower:lower + shard], preferred_element_type=jnp.float32)
        rounded = lax.optimization_barrier(part.astype(jnp.bfloat16))
        projected = projected + rounded.astype(jnp.float32)
    mixer_output = scale_rows(projected, mix_gain).astype(jnp.bfloat16)
    normed = scale_rows(moe_input.astype(jnp.float32), in_gain).astype(jnp.bfloat16)
    group_logits = jnp.dot(normed, group_router, preferred_element_type=jnp.float32)
    expert_logits = jnp.dot(normed, expert_router, preferred_element_type=jnp.float32)
    per_group = EXPERTS // GROUPS
    expert_match = routes[:, :, None] == jnp.arange(EXPERTS, dtype=jnp.int32)[None, None, :]
    picked_logits = lax.optimization_barrier(jnp.sum(jnp.where(expert_match, expert_logits[:, None, :], 0.0), axis=-1))
    group_prob = jax.nn.softmax(group_logits, axis=-1)
    group_match = (routes // per_group)[:, :, None] == jnp.arange(GROUPS, dtype=jnp.int32)[None, None, :]
    picked_group = lax.optimization_barrier(jnp.sum(jnp.where(group_match, group_prob[:, None, :], 0.0), axis=-1))
    route_weight = picked_group * jax.nn.softmax(picked_logits, axis=-1)
    blocks = TOKENS // TOK_DEV
    match_int = expert_match.astype(jnp.int32).reshape(blocks, TOK_DEV * TOP, EXPERTS)
    before = jnp.cumsum(match_int, axis=1) - match_int
    slot = lax.optimization_barrier(jnp.sum(before * match_int, axis=-1)).reshape(TOKENS, TOP)
    block_of = (jnp.arange(TOKENS, dtype=jnp.int32) // TOK_DEV)[:, None]
    column = (block_of * CAP + slot).astype(jnp.int32)
    token_ids = jnp.broadcast_to(jnp.arange(TOKENS, dtype=jnp.int32)[:, None], (TOKENS, TOP))
    table = jnp.full((EXPERTS, blocks * CAP), TOKENS, jnp.int32)
    table = table.at[routes.reshape(-1), column.reshape(-1)].set(token_ids.reshape(-1))
    weight_table = jnp.zeros((EXPERTS, blocks * CAP), jnp.float32)
    weight_table = weight_table.at[routes.reshape(-1), column.reshape(-1)].set(route_weight.reshape(-1))
    padded = jnp.concatenate([normed, jnp.zeros((1, D), normed.dtype)], axis=0)

    def one_expert(running, expert):
        index = table[expert]
        rows = jnp.take(padded, index, axis=0)
        gate = jnp.dot(rows, gate_weight[expert], preferred_element_type=jnp.float32)
        up = jnp.dot(rows, up_weight[expert], preferred_element_type=jnp.float32)
        hidden = (jax.nn.silu(gate) * up).astype(jnp.bfloat16)
        expert_rows = jnp.dot(hidden, down_weight[expert].T, preferred_element_type=jnp.float32).astype(jnp.bfloat16)
        weighted = weight_table[expert][:, None] * expert_rows.astype(jnp.float32)
        return (running.at[index].add(weighted, mode='drop'), None)
    moe, unused = lax.scan(one_expert, jnp.zeros((TOKENS, D), jnp.float32), jnp.arange(EXPERTS, dtype=jnp.int32))
    moe_output = scale_rows(moe, out_gain).astype(jnp.bfloat16)
    return (mixer_output, moe_output)
```

```python
import math

import jax
import jax.numpy as jnp
from jax import lax
from jax.sharding import PartitionSpec as P

HEADS = 16
HD = 64
KV_HEADS = 4
WINDOW = 128
CORES = 2


eps = 1e-06


def shifted(block, axis, distance):
    devices = range(lax.axis_size(axis))
    route = [(i - distance, i) for i in devices if i - distance in devices]
    return lax.ppermute(block, axis, route)


def swapped(block, axis, bit):
    route = [(i, i ^ bit) for i in range(lax.axis_size(axis))]
    return lax.ppermute(block, axis, route)


def bits_of(axis):
    return [1 << i for i in range((lax.axis_size(axis) - 1).bit_length())]


def gathered(block, axis, order):
    held = {0: block}
    for bit in order:
        held.update({offset ^ bit: swapped(held[offset], axis, bit) for offset in list(held)})
    return [held[offset] for offset in range(lax.axis_size(axis))]


def gathered_joined(block, axis, order):
    offsets = [0]
    joined = block[None]
    for bit in order:
        joined = jnp.concatenate([joined, swapped(joined, axis, bit)], axis=0)
        offsets = offsets + [offset ^ bit for offset in offsets]
    return joined, offsets


def scale_rows(matrix, gain):
    mean_square = jnp.mean(matrix * matrix, axis=-1, keepdims=True)
    return matrix * lax.rsqrt(mean_square + eps) * gain


def attend(queries, keys, values, slopes, sinks):
    rows_group = queries.shape[0]
    local_heads = slopes.shape[0]
    per_kv = HEADS // KV_HEADS
    kv_index = lax.axis_index("tp") * local_heads // per_kv
    own_keys = lax.dynamic_slice_in_dim(keys, kv_index * HD, HD, 1)
    own_values = lax.dynamic_slice_in_dim(values, kv_index * HD, HD, 1)
    rim = jnp.concatenate(
        [own_keys[rows_group - WINDOW :], own_values[rows_group - WINDOW :]], axis=1
    )
    rim = shifted(rim, "ep", 1)
    rim_keys, rim_values = rim[:, :HD], rim[:, HD:]
    blocks = rows_group // WINDOW
    key_blocks = own_keys.reshape(blocks, WINDOW, HD)
    value_blocks = own_values.reshape(blocks, WINDOW, HD)
    key_span = jnp.concatenate(
        [jnp.concatenate([rim_keys[None], key_blocks[:-1]], axis=0), key_blocks], axis=1
    )
    value_span = jnp.concatenate(
        [jnp.concatenate([rim_values[None], value_blocks[:-1]], axis=0), value_blocks], axis=1
    )
    query_blocks = queries.reshape(blocks, WINDOW, local_heads, HD)
    scores = jnp.einsum(
        "nqhd,nsd->nhqs", query_blocks, key_span, preferred_element_type=jnp.float32
    ) * (1.0 / math.sqrt(HD))
    query_index = jnp.arange(WINDOW, dtype=jnp.int32)[:, None]
    key_index = jnp.arange(2 * WINDOW, dtype=jnp.int32)[None, :]
    distance = query_index + WINDOW - key_index
    key_position = (
        lax.axis_index("ep") * rows_group
        + jnp.arange(blocks, dtype=jnp.int32)[:, None, None] * WINDOW
        + key_index[None]
        - WINDOW
    )
    valid = ((distance >= 0) & (distance < WINDOW))[None] & (key_position >= 0)
    scores = scores - slopes[None, :, None, None] * distance.astype(jnp.float32)[None, None]
    scores = jnp.where(valid[:, None], scores, -jnp.inf)
    sink = sinks[None, :, None, None]
    top = jnp.maximum(jnp.max(scores, axis=-1, keepdims=True), sink)
    weights = jnp.exp(scores - top)
    denom = jnp.sum(weights, axis=-1, keepdims=True) + jnp.exp(sink - top)
    probs = (weights / denom).astype(jnp.bfloat16)
    attention = jnp.einsum("nhqs,nsd->nqhd", probs, value_span, preferred_element_type=jnp.float32)
    return attention.astype(jnp.bfloat16).reshape(rows_group, local_heads * HD)


def route_table(normed, group_router, expert_router, routes):
    group_logits = jnp.dot(normed, group_router, preferred_element_type=jnp.float32)
    expert_logits = jnp.dot(normed, expert_router, preferred_element_type=jnp.float32)
    experts = expert_router.shape[1]
    groups = group_router.shape[1]
    per_group = experts // groups
    expert_match = routes[:, :, None] == jnp.arange(experts, dtype=jnp.int32)[None, None, :]
    picked_logits = jnp.sum(jnp.where(expert_match, expert_logits[:, None, :], 0.0), axis=-1)
    group_prob = jax.nn.softmax(group_logits, axis=-1)
    group_match = (routes // per_group)[:, :, None] == jnp.arange(groups, dtype=jnp.int32)[
        None, None, :
    ]
    picked_group = jnp.sum(jnp.where(group_match, group_prob[:, None, :], 0.0), axis=-1)
    route_weight = picked_group * jax.nn.softmax(picked_logits, axis=-1)
    return jnp.sum(jnp.where(expert_match, route_weight[:, :, None], 0.0), axis=1)


def per_device(
    queries,
    keys,
    values,
    slopes,
    sinks,
    out_weight,
    mix_gain,
    moe_input,
    in_gain,
    out_gain,
    group_router,
    expert_router,
    routes,
    gate_weight,
    up_weight,
    down_weight,
):
    size_ep, size_tp = lax.axis_size("ep"), lax.axis_size("tp")
    me_ep, me_tp = lax.axis_index("ep"), lax.axis_index("tp")
    ep_bits, tp_bits = bits_of("ep"), bits_of("tp")
    forth, back = ep_bits, ep_bits[::-1]
    own_rows, width = moe_input.shape
    half = width // 2
    gates = gathered(gate_weight, "ep", forth)
    ups = gathered(up_weight, "ep", back)
    downs_low = gathered(down_weight[:, :half], "ep", forth)
    downs_high = gathered(down_weight[:, half:], "ep", back)

    normed = scale_rows(moe_input.astype(jnp.float32), in_gain).astype(jnp.bfloat16)
    tokens, offsets = gathered_joined(normed, "tp", tp_bits[::-1])
    table = route_table(normed, group_router, expert_router, routes)
    tables, _ = gathered_joined(table, "tp", tp_bits[::-1])
    tokens = tokens.reshape(size_tp * own_rows, width)
    tables = tables.reshape(size_tp * own_rows, -1)

    attention = attend(queries, keys, values, slopes, sinks)
    pieces = lax.all_to_all(
        attention.reshape(size_tp, own_rows, -1), "tp", split_axis=0, concat_axis=0, tiled=True
    )
    columns = width // size_ep
    share = lax.dynamic_slice_in_dim(out_weight, me_ep * columns, columns, 1)
    share, share_offsets = gathered_joined(share, "tp", tp_bits[::-1])
    pieces = jnp.take(pieces, me_tp ^ jnp.array(share_offsets, jnp.int32), axis=0)
    pieces = pieces.transpose(1, 0, 2).reshape(own_rows, -1)
    share = share.reshape(-1, columns)
    cut = share.shape[0] // 2
    shares_low = gathered(share[:cut], "ep", forth)
    shares_high = gathered(share[cut:], "ep", back)
    projected = jnp.stack(
        [
            jnp.dot(pieces[:, :cut], low, preferred_element_type=jnp.float32)
            + jnp.dot(pieces[:, cut:], high, preferred_element_type=jnp.float32)
            for low, high in zip(shares_low, shares_high)
        ]
    )
    projected = jnp.take(projected, me_ep ^ jnp.arange(size_ep, dtype=jnp.int32), axis=0)
    projected = projected.transpose(1, 0, 2).reshape(own_rows, width)
    mixer_output = scale_rows(projected, mix_gain).astype(jnp.bfloat16)

    hidden = []
    local = gate_weight.shape[0]
    for offset, (gate, up) in enumerate(zip(gates, ups)):
        for inner in range(local):
            gated = jnp.dot(tokens, gate[inner], preferred_element_type=jnp.float32)
            upped = jnp.dot(tokens, up[inner], preferred_element_type=jnp.float32)
            expert = (me_ep ^ offset) * local + inner
            amount = lax.dynamic_slice_in_dim(tables, expert, 1, 1)
            product = jax.nn.silu(gated) * upped * amount
            hidden.append(jnp.where(amount > 0, product, 0.0).astype(jnp.bfloat16))
    hidden = jnp.concatenate(hidden, axis=1)
    results = []
    for downs in (downs_low, downs_high):
        down = jnp.concatenate([d[inner] for d in downs for inner in range(local)], axis=1)
        part = jnp.einsum("tf,df->td", hidden, down, preferred_element_type=jnp.float32)
        part = part.reshape(size_tp, own_rows, half)
        for bit in tp_bits[:1] + tp_bits[1:]:
            count = part.shape[0] // 2
            got = swapped(part[count:].astype(jnp.bfloat16), "tp", bit)
            part = part[:count] + got.astype(jnp.float32)
        results.append(part[0])
    moe = jnp.concatenate(results, axis=1)
    moe_output = scale_rows(moe, out_gain).astype(jnp.bfloat16)
    return (mixer_output, moe_output)


def solution(mesh):
    return jax.shard_map(
        per_device,
        mesh=mesh,
        in_specs=(
            P("ep", "tp"),
            P("ep", None),
            P("ep", None),
            P("tp"),
            P("tp"),
            P("tp", None),
            P(),
            P(("ep", "tp"), None),
            P(),
            P(),
            P(),
            P(),
            P(("ep", "tp"), None),
            P("ep", None, "tp"),
            P("ep", None, "tp"),
            P("ep", None, "tp"),
        ),
        out_specs=(P(("ep", "tp"), None), P(("ep", "tp"), None)),
        check_vma=False,
    )
```

```python
import functools
import math

import jax
import jax.numpy as jnp
from jax import lax
from jax.experimental import pallas as pl
from jax.experimental.pallas import tpu as pltpu
from jax.sharding import PartitionSpec as P

HEADS = 16
HD = 64
KV_HEADS = 4
WINDOW = 128
CHUNKS = 4


eps = 1e-06
MESH = pl.DeviceIdType.MESH
F32 = jnp.float32
BF16 = jnp.bfloat16


def flipped(index, bit):
    return index + bit - 2 * bit * ((index // bit) % 2)


def partner_of(index, offset, size):
    bit = 1
    while bit < size:
        if offset & bit:
            index = flipped(index, bit)
        bit *= 2
    return index


def bits_of(size):
    return [1 << i for i in range((size - 1).bit_length())]


def offsets_of(order):
    offsets = [0]
    for bit in order:
        offsets = offsets + [offset ^ bit for offset in offsets]
    return offsets


def scale_rows(matrix, gain):
    mean_square = jnp.mean(matrix * matrix, axis=-1, keepdims=True)
    return matrix * lax.rsqrt(mean_square + eps) * gain


def kernel(
    n_ep,
    n_tp,
    queries,
    keys,
    values,
    slopes,
    sinks,
    out_weight,
    mix_gain,
    moe_input,
    in_gain,
    out_gain,
    group_router,
    expert_router,
    routes,
    gate_weight,
    up_weight,
    down_weight,
    mixer_output,
    moe_output,
    gates,
    ups,
    downs,
    tokens,
    tables,
    key_rows,
    value_rows,
    attended,
    pieces,
    share,
    projected,
    hidden,
    landed,
    total,
    local_sem,
    ep_send,
    ep_recv,
    tp_send,
    tp_recv,
    rs_send,
    rs_recv,
):
    me_ep, me_tp = lax.axis_index("ep"), lax.axis_index("tp")
    rows, width = moe_input.shape
    local, _, units = gate_weight.shape
    group_rows = rows * n_tp
    columns = width // n_ep
    chunk = width // CHUNKS
    half_chunk = chunk // 2
    forth = bits_of(n_ep)
    back = forth[::-1]
    tp_order = bits_of(n_tp)[::-1]
    tp_offsets = offsets_of(tp_order)
    cut = group_rows_cut = share.shape[1] // 2

    sent = []
    locals_ = []

    def local_copy(source, target):
        copy = pltpu.make_async_copy(source, target, local_sem.at[len(locals_)])
        copy.start()
        locals_.append(copy)
        return copy

    def send(source, target, send_sem, recv_sem, where):
        copy = pltpu.make_async_remote_copy(
            src_ref=source,
            dst_ref=target,
            send_sem=send_sem,
            recv_sem=recv_sem,
            device_id=where,
            device_id_type=MESH,
        )
        copy.start()
        sent.append(copy)
        return copy

    class Spread:
        def __init__(self, number, own, slot_of, order):
            self.number, self.own, self.slot_of, self.order = number, own, slot_of, order
            self.coming = {}
            self.ready = {0}

        def post(self, source, offset, bit):
            target = offset ^ bit
            self.coming[target] = send(
                source,
                self.slot_of(target),
                ep_send.at[self.number, target],
                ep_recv.at[self.number, target],
                {"ep": flipped(me_ep, bit)},
            )

        def first(self, step):
            self.post(self.own, 0, self.order[step])

        def wait(self, offset):
            if offset not in self.ready:
                self.coming[offset].wait_recv()
                self.ready.add(offset)

        def forward(self):
            held = [0]
            for bit in self.order:
                for offset in held:
                    if offset:
                        self.wait(offset)
                        self.post(self.slot_of(offset), offset, bit)
                held = held + [offset ^ bit for offset in held]

    gate_spread = Spread(0, gate_weight, lambda o: gates.at[o], forth)
    up_spread = Spread(1, up_weight, lambda o: ups.at[o], back)
    down_spreads = []
    for c in range(CHUNKS):
        for part, order in ((0, forth), (1, back)):
            span = pl.ds(c * chunk + part * half_chunk, half_chunk)
            down_spreads.append(
                Spread(
                    2 + 2 * c + part,
                    down_weight.at[:, span],
                    lambda o, span=span: downs.at[o, :, span],
                    order,
                )
            )
    share_spreads = [
        Spread(
            2 + 2 * CHUNKS + part,
            share.at[0, pl.ds(part * cut, cut)],
            lambda o, part=part: share.at[o, pl.ds(part * cut, cut)],
            order,
        )
        for part, order in ((0, forth), (1, back))
    ]
    halo_number = 4 + 2 * CHUNKS

    take_keys = local_copy(keys, key_rows.at[pl.ds(WINDOW, group_rows)])
    take_values = local_copy(values, value_rows.at[pl.ds(WINDOW, group_rows)])
    take_gate = local_copy(gate_weight, gates.at[0])
    take_up = local_copy(up_weight, ups.at[0])
    take_down = local_copy(down_weight, downs.at[0])
    own_columns = pl.ds(pl.multiple_of(me_ep * columns, columns), columns)
    take_share = local_copy(out_weight.at[:, own_columns], share.at[0, pl.ds(0, out_weight.shape[0])])

    ep_next = lax.rem(me_ep + 1, n_ep)
    ep_prev = lax.rem(me_ep + n_ep - 1, n_ep)
    barrier = pltpu.get_barrier_semaphore()
    greeted = [{"tp": partner_of(me_tp, offset, n_tp)} for offset in range(1, n_tp)]
    greeted += [{"ep": flipped(me_ep, bit)} for bit in forth]
    greeted += [{"ep": ep_next}, {"ep": ep_prev}]
    for where in greeted:
        pl.semaphore_signal(barrier, inc=1, device_id=where, device_id_type=MESH)
    pl.semaphore_wait(barrier, len(greeted))

    halo = []
    last_rows = pl.ds(group_rows - WINDOW, WINDOW)
    for place, (source, target) in enumerate(((keys, key_rows), (values, value_rows))):
        halo.append(
            send(
                source.at[last_rows],
                target.at[pl.ds(0, WINDOW)],
                ep_send.at[halo_number + place, 0],
                ep_recv.at[halo_number + place, 0],
                {"ep": ep_next},
            )
        )
    for step in range(len(forth)):
        gate_spread.first(step)
        up_spread.first(step)

    normed = scale_rows(moe_input[...].astype(F32), in_gain[...]).astype(BF16)
    tokens[pl.ds(0, rows)] = normed
    coming = {}
    token_ready = {0}

    def span_of(position):
        return pl.ds(position * rows, rows)

    def token_send(position, step):
        target = position + (1 << step)
        coming[target] = send(
            tokens.at[span_of(position)],
            tokens.at[span_of(target)],
            tp_send.at[0, target],
            tp_recv.at[0, target],
            {"tp": flipped(me_tp, tp_order[step])},
        )

    def token_wait(position):
        if position not in token_ready:
            coming[position].wait_recv()
            token_ready.add(position)

    steps = len(tp_order)
    for step in reversed(range(steps)):
        token_send(0, step)

    def to_all(number, source_of, target_of):
        waits = []
        for position in range(1, n_tp):
            other = partner_of(me_tp, tp_offsets[position], n_tp)
            waits.append(
                send(
                    source_of(other),
                    target_of(position),
                    tp_send.at[number, position],
                    tp_recv.at[number, position],
                    {"tp": other},
                )
            )
        return waits

    group_logits = jnp.dot(normed, group_router[...], preferred_element_type=F32)
    expert_logits = jnp.dot(normed, expert_router[...], preferred_element_type=F32)
    experts, groups = expert_logits.shape[1], group_logits.shape[1]
    per_group = experts // groups
    group_shifted = jnp.exp(group_logits - jnp.max(group_logits, axis=-1, keepdims=True))
    group_prob = group_shifted / jnp.sum(group_shifted, axis=-1, keepdims=True)
    expert_ids = lax.broadcasted_iota(jnp.int32, (rows, experts), 1)
    group_ids = lax.broadcasted_iota(jnp.int32, (rows, groups), 1)
    visited = [routes[:, k : k + 1] for k in range(routes.shape[1])]
    matches = [expert_ids == visit for visit in visited]
    picked = [
        jnp.sum(jnp.where(match, expert_logits, 0.0), axis=-1, keepdims=True) for match in matches
    ]
    highest = functools.reduce(jnp.maximum, picked)
    picked = [jnp.exp(p - highest) for p in picked]
    picked_sum = functools.reduce(jnp.add, picked)
    table = jnp.zeros((rows, experts), F32)
    for visit, match, p in zip(visited, matches, picked):
        chosen = jnp.zeros((rows, 1), F32)
        for g in range(groups):
            inside = (visit >= g * per_group) & (visit < (g + 1) * per_group)
            chosen = chosen + jnp.where(inside, group_prob[:, g : g + 1], 0.0)
        table = table + jnp.where(match, chosen * (p / picked_sum), 0.0)
    padded = jnp.concatenate([table, jnp.zeros((rows, rows - experts), F32)], axis=1)
    tables[0] = padded.T[: tables.shape[1]]
    table_waits = to_all(1, lambda other: tables.at[0], lambda position: tables.at[position])

    take_keys.wait()
    take_values.wait()
    for copy in halo:
        copy.wait_recv()
    local_heads = slopes.shape[0]
    per_kv = HEADS // KV_HEADS

    def attend_block(block, carry):
        start = pl.multiple_of(block * WINDOW, WINDOW)
        q = queries[pl.ds(start, WINDOW)]
        k = key_rows[pl.ds(start, 2 * WINDOW)]
        v = value_rows[pl.ds(start, 2 * WINDOW)]
        query_index = lax.broadcasted_iota(jnp.int32, (WINDOW, 2 * WINDOW), 0)
        key_index = lax.broadcasted_iota(jnp.int32, (WINDOW, 2 * WINDOW), 1)
        distance = query_index + WINDOW - key_index
        position = me_ep * group_rows + start + key_index - WINDOW
        valid = (distance >= 0) & (distance < WINDOW) & (position >= 0)
        far = distance.astype(F32)
        outs = []
        for h in range(local_heads):
            kv = (me_tp * local_heads + h) // per_kv
            own = q[:, h * HD : (h + 1) * HD]
            nothing = jnp.zeros_like(own)
            spread = jnp.concatenate(
                [jnp.where(kv == i, own, nothing) for i in range(KV_HEADS)], axis=1
            )
            scores = lax.dot_general(
                spread, k, (((1,), (1,)), ((), ())), preferred_element_type=F32
            ) * (1.0 / math.sqrt(HD))
            scores = jnp.where(valid, scores - slopes[h] * far, -jnp.inf)
            top = jnp.maximum(jnp.max(scores, axis=-1, keepdims=True), sinks[h])
            weights = jnp.exp(scores - top)
            denom = jnp.sum(weights, axis=-1, keepdims=True) + jnp.exp(sinks[h] - top)
            probs = (weights / denom).astype(BF16)
            mixed = jnp.dot(probs, v, preferred_element_type=F32)
            outs.append(
                sum(
                    jnp.where(kv == i, mixed[:, i * HD : (i + 1) * HD], 0.0)
                    for i in range(KV_HEADS)
                )
            )
        joined = outs[0] if local_heads == 1 else jnp.concatenate(outs, axis=1)
        attended[pl.ds(start, WINDOW)] = joined.astype(BF16)
        return carry

    lax.fori_loop(0, group_rows // WINDOW, attend_block, 0)

    def attended_of(index):
        return pl.ds(pl.multiple_of(index * rows, rows), rows)

    piece_waits = to_all(
        2, lambda other: attended.at[attended_of(other)], lambda position: pieces.at[position]
    )
    pieces[0] = attended[attended_of(me_tp)]

    gate_spread.forward()
    up_spread.forward()
    for spread in down_spreads[:4]:
        for step in range(len(forth)):
            spread.first(step)
    for step in range(1, steps):
        for position in range(1, 1 << step):
            token_wait(position)
            token_send(position, step)
    take_share.wait()
    share_rows = out_weight.shape[0]
    share_waits = {}

    def share_send(position, step):
        target = position + (1 << step)
        share_waits[target] = send(
            share.at[0, pl.ds(position * share_rows, share_rows)],
            share.at[0, pl.ds(target * share_rows, share_rows)],
            tp_send.at[3, target],
            tp_recv.at[3, target],
            {"tp": flipped(me_tp, tp_order[step])},
        )

    share_ready = {0}

    def share_wait(position):
        if position not in share_ready:
            share_waits[position].wait_recv()
            share_ready.add(position)

    for step in range(steps):
        share_send(0, step)

    take_gate.wait()
    take_up.wait()
    for copy in table_waits:
        copy.wait_recv()

    def hidden_part(offset, inner, first, count):
        span = pl.ds(first * rows, count * rows)
        weight = jnp.concatenate([gates[offset, inner], ups[offset, inner]], axis=1)
        both = jnp.dot(tokens[span], weight, preferred_element_type=F32)
        gated, upped = both[:, :units], both[:, units:]
        expert = partner_of(me_ep, offset, n_ep) * local + inner
        amounts = []
        for position in range(first, first + count):
            block = tables[position]
            expert_row = lax.broadcasted_iota(jnp.int32, block.shape, 0)
            line = jnp.sum(jnp.where(expert_row == expert, block, 0.0), axis=0, keepdims=True)
            amounts.append(jnp.broadcast_to(line, (rows, rows)).T)
        amount = jnp.concatenate(amounts, axis=0)[:, :units]
        product = gated / (1.0 + jnp.exp(-gated)) * upped * amount
        product = jnp.where(amount > 0, product, 0.0).astype(BF16)
        place = (offset * local + inner) * units
        hidden[span, place : place + units] = product

    side = n_tp // 2
    early = n_tp // 4 + 1
    ranges = [(0, early), (side, early), (early, side - early), (side + early, side - early)]

    def hidden_parts(offset, wanted):
        gate_spread.wait(offset)
        up_spread.wait(offset)
        for first, count in wanted:
            for position in range(first, first + count):
                token_wait(position)
            for inner in range(local):
                hidden_part(offset, inner, first, count)

    for offset in range(n_ep - 1):
        hidden_parts(offset, ranges[:2])
    for step in range(1, steps):
        for position in range(1, 1 << step):
            share_wait(position)
            share_send(position, step)
    for spread in down_spreads[:2]:
        spread.forward()
    for spread in down_spreads[4:]:
        for step in range(len(forth)):
            spread.first(step)
    for offset in range(n_ep - 1):
        hidden_parts(offset, ranges[2:])
    hidden_parts(n_ep - 1, [(0, side), (side, side)])

    take_down.wait()
    rs_order = tp_order[::-1]
    arrivals = {}
    for copy in sent:
        pass
    token_copies = [coming[position] for position in coming]
    for copy in token_copies:
        copy.wait_send()
    waited = set(id(copy) for copy in token_copies)

    def columns_of(c):
        return pl.ds(c * chunk, chunk)

    def down_of(c):
        return jnp.concatenate(
            [
                downs[offset, inner, c * chunk : (c + 1) * chunk]
                for offset in range(n_ep)
                for inner in range(local)
            ],
            axis=1,
        )

    def down_dot(c, first, count):
        return lax.dot_general(
            hidden[pl.ds(first * rows, count * rows)],
            down_of(c),
            (((1,), (1,)), ((), ())),
            preferred_element_type=F32,
        )

    def reduce_send(c, step):
        count = n_tp >> (step + 1)
        source = tokens.at[pl.ds(count * rows, count * rows), columns_of(c)]
        target = landed.at[pl.ds((count - 1) * rows, count * rows), columns_of(c)]
        arrivals[c, step] = send(
            source,
            target,
            rs_send.at[c, step],
            rs_recv.at[c, step],
            {"tp": flipped(me_tp, rs_order[step])},
        )

    def arrived(c, step):
        count = n_tp >> (step + 1)
        arrivals[c, step].wait_recv()
        return landed[pl.ds((count - 1) * rows, count * rows), columns_of(c)].astype(F32)

    def keep(c, value, count):
        upper = count // 2
        if count > 1:
            tokens[pl.ds(upper * rows, upper * rows), columns_of(c)] = value[upper * rows :].astype(
                BF16
            )
            total[pl.ds(0, upper * rows), columns_of(c)] = value[: upper * rows]
        else:
            total[pl.ds(0, rows), columns_of(c)] = value

    def reduce_open(c):
        for spread in down_spreads[2 * c : 2 * c + 2]:
            for offset in range(1, n_ep):
                spread.wait(offset)
        tokens[pl.ds(side * rows, side * rows), columns_of(c)] = down_dot(c, side, side).astype(BF16)
        reduce_send(c, 0)

    def reduce_second(c):
        value = down_dot(c, 0, side)
        keep(c, value + arrived(c, 0), side)
        reduce_send(c, 1)

    def reduce_step(c, step):
        count = n_tp >> (step + 1)
        keep(c, total[pl.ds(0, count * rows), columns_of(c)] + arrived(c, step), count)
        if step + 1 < steps:
            reduce_send(c, step + 1)

    def project(offset):
        for spread in share_spreads:
            spread.wait(offset)
        joined = jnp.concatenate([pieces[position] for position in range(n_tp)], axis=1)
        place = pl.multiple_of(partner_of(me_ep, offset, n_ep) * columns, columns)
        projected[:, pl.ds(place, columns)] = jnp.dot(
            joined, share[offset], preferred_element_type=F32
        )

    later = [(c, step) for c in range(CHUNKS) for step in range(2, steps)]

    reduce_open(0)
    reduce_second(0)
    for spread in down_spreads[2:4]:
        spread.forward()
    reduce_open(1)
    reduce_second(1)
    for spread in down_spreads[4:6]:
        spread.forward()
    for position in range(1, n_tp):
        share_wait(position)
    for spread in share_spreads:
        for step in range(len(forth)):
            spread.first(step)
    reduce_step(0, 1)
    reduce_open(2)
    reduce_second(2)
    for spread in down_spreads[6:8]:
        spread.forward()
    reduce_step(1, 1)
    reduce_open(3)
    reduce_second(3)
    for spread in share_spreads:
        spread.forward()
    reduce_step(2, 1)
    for step in range(2, steps):
        reduce_step(0, step)
    reduce_step(3, 1)
    for copy in piece_waits:
        copy.wait_recv()
    for offset in range(n_ep):
        project(offset)
    mixer_output[...] = scale_rows(projected[...], mix_gain[...]).astype(BF16)
    for c in range(1, CHUNKS):
        for step in range(2, steps):
            reduce_step(c, step)
    moe_output[...] = scale_rows(total[pl.ds(0, rows)], out_gain[...]).astype(BF16)

    for copy in sent:
        if id(copy) not in waited:
            copy.wait_send()


def per_device(n_ep, n_tp, *arguments):
    (queries, keys, values, slopes, sinks, out_weight, mix_gain, moe_input, in_gain, out_gain) = (
        arguments[:10]
    )
    group_router, expert_router, routes, gate_weight, up_weight, down_weight = arguments[10:]
    rows, width = moe_input.shape
    group_rows = rows * n_tp
    local, _, units = gate_weight.shape
    columns = width // n_ep
    experts = expert_router.shape[1]
    whole = pl.BlockSpec(memory_space=pltpu.VMEM)
    scalar = pl.BlockSpec(memory_space=pltpu.SMEM)
    outside = pl.BlockSpec(memory_space=pl.ANY)
    steps = (n_tp - 1).bit_length()
    copies = 6 + 2 * CHUNKS
    return pl.pallas_call(
        functools.partial(kernel, n_ep, n_tp),
        out_shape=[jax.ShapeDtypeStruct((rows, width), BF16)] * 2,
        in_specs=[
            whole,
            outside,
            outside,
            scalar,
            scalar,
            outside,
            whole,
            whole,
            whole,
            whole,
            whole,
            whole,
            whole,
            outside,
            outside,
            outside,
        ],
        out_specs=[whole, whole],
        scratch_shapes=[
            pltpu.VMEM((n_ep, local, width, units), BF16),
            pltpu.VMEM((n_ep, local, width, units), BF16),
            pltpu.VMEM((n_ep, local, width, units), BF16),
            pltpu.VMEM((group_rows, width), BF16),
            pltpu.VMEM((n_tp, max(8, experts), rows), F32),
            pltpu.VMEM((WINDOW + group_rows, keys.shape[1]), BF16),
            pltpu.VMEM((WINDOW + group_rows, values.shape[1]), BF16),
            pltpu.VMEM(queries.shape, BF16),
            pltpu.VMEM((n_tp, rows, queries.shape[1]), BF16),
            pltpu.VMEM((n_ep, out_weight.shape[0] * n_tp, columns), BF16),
            pltpu.VMEM((rows, width), F32),
            pltpu.VMEM((group_rows, n_ep * local * units), BF16),
            pltpu.VMEM((group_rows - rows, width), BF16),
            pltpu.VMEM((group_rows // 4, width), F32),
            pltpu.SemaphoreType.DMA((8,)),
            pltpu.SemaphoreType.DMA((copies, n_ep)),
            pltpu.SemaphoreType.DMA((copies, n_ep)),
            pltpu.SemaphoreType.DMA((4, n_tp)),
            pltpu.SemaphoreType.DMA((4, n_tp)),
            pltpu.SemaphoreType.DMA((CHUNKS, steps)),
            pltpu.SemaphoreType.DMA((CHUNKS, steps)),
        ],
        compiler_params=pltpu.CompilerParams(
            collective_id=0, has_side_effects=True, vmem_limit_bytes=67000000
        ),
    )(
        queries,
        keys,
        values,
        slopes,
        sinks,
        out_weight,
        mix_gain[None],
        moe_input,
        in_gain[None],
        out_gain[None],
        group_router,
        expert_router,
        routes,
        gate_weight,
        up_weight,
        down_weight,
    )


def solution(mesh):
    return jax.shard_map(
        functools.partial(per_device, mesh.shape["ep"], mesh.shape["tp"]),
        mesh=mesh,
        in_specs=(
            P("ep", "tp"),
            P("ep", None),
            P("ep", None),
            P("tp"),
            P("tp"),
            P("tp", None),
            P(),
            P(("ep", "tp"), None),
            P(),
            P(),
            P(),
            P(),
            P(("ep", "tp"), None),
            P("ep", None, "tp"),
            P("ep", None, "tp"),
            P("ep", None, "tp"),
        ),
        out_specs=(P(("ep", "tp"), None), P(("ep", "tp"), None)),
        check_vma=False,
    )
```

```python
import functools
import math

import jax
import jax.numpy as jnp
from jax import lax
from jax.experimental import pallas as pl
from jax.experimental.pallas import tpu as pltpu
from jax.sharding import PartitionSpec as P

HEADS = 16
HD = 64
KV_HEADS = 4
WINDOW = 128
CHUNKS = 8
LAG = 2
SHARE_FIRST = 2
SHARE_ON = 6


eps = 1e-06
MESH = pl.DeviceIdType.MESH
F32 = jnp.float32
BF16 = jnp.bfloat16


def flipped(index, bit):
    return index + bit - 2 * bit * ((index // bit) % 2)


def partner_of(index, offset, size):
    bit = 1
    while bit < size:
        if offset & bit:
            index = flipped(index, bit)
        bit *= 2
    return index


def bits_of(size):
    return [1 << i for i in range((size - 1).bit_length())]


def offsets_of(order):
    offsets = [0]
    for bit in order:
        offsets = offsets + [offset ^ bit for offset in offsets]
    return offsets


def scale_rows(matrix, gain):
    mean_square = jnp.mean(matrix * matrix, axis=-1, keepdims=True)
    return matrix * lax.rsqrt(mean_square + eps) * gain


def kernel(
    n_ep,
    n_tp,
    queries_out,
    keys,
    values,
    slopes,
    sinks,
    out_weight,
    moe_input_out,
    in_gain_out,
    group_router_out,
    expert_router_out,
    routes_out,
    gate_weight,
    up_weight,
    down_weight,
    projected,
    total,
    queries,
    in_gain,
    group_router,
    expert_router,
    routes,
    gates,
    ups,
    downs,
    tokens,
    tables,
    key_rows,
    value_rows,
    pieces,
    share,
    hidden,
    landed,
    held,
    local_sem,
    ep_send,
    ep_recv,
    tp_send,
    tp_recv,
    rs_send,
    rs_recv,
):
    me_ep, me_tp = lax.axis_index("ep"), lax.axis_index("tp")
    rows, width = moe_input_out.shape
    local, _, units = gate_weight.shape
    group_rows = rows * n_tp
    columns = width // n_ep
    chunk = width // CHUNKS
    forth = bits_of(n_ep)
    back = forth[::-1]
    tp_order = bits_of(n_tp)[::-1]
    tp_offsets = offsets_of(tp_order)
    cut = share.shape[1] // 4

    sent = []
    locals_ = []

    class Tracked:
        def __init__(self, copy):
            self.copy, self.gone, self.here = copy, False, False

        def start(self):
            self.copy.start()

        def wait_send(self):
            if not self.gone:
                self.copy.wait_send()
                self.gone = True

        def wait_recv(self):
            if not self.here:
                self.copy.wait_recv()
                self.here = True

    def local_copy(source, target):
        copy = pltpu.make_async_copy(source, target, local_sem.at[len(locals_)])
        copy.start()
        locals_.append(copy)
        return copy

    def send(source, target, send_sem, recv_sem, where, started=True):
        copy = pltpu.make_async_remote_copy(
            src_ref=source,
            dst_ref=target,
            send_sem=send_sem,
            recv_sem=recv_sem,
            device_id=where,
            device_id_type=MESH,
        )
        if started:
            copy.start()
        sent.append(Tracked(copy))
        return sent[-1]

    class Spread:
        def __init__(self, number, own, slot_of, order):
            self.number, self.own, self.slot_of, self.order = number, own, slot_of, order
            self.coming = {}

        def post(self, source, offset, bit):
            target = offset ^ bit
            self.coming[target] = send(
                source,
                self.slot_of(target),
                ep_send.at[self.number, target],
                ep_recv.at[self.number, target],
                {"ep": flipped(me_ep, bit)},
            )

        def first(self, step):
            self.post(self.own, 0, self.order[step])

        def wait(self, offset):
            if offset:
                self.coming[offset].wait_recv()

        def forward(self):
            held = [0]
            for bit in self.order:
                for offset in held:
                    if offset:
                        self.wait(offset)
                        self.post(self.slot_of(offset), offset, bit)
                held = held + [offset ^ bit for offset in held]

    gate_spread = Spread(0, gate_weight, lambda o: gates.at[o], forth)
    up_spread = Spread(1, up_weight, lambda o: ups.at[o], back)
    share_spreads = [
        Spread(
            2 + part,
            share.at[0, pl.ds(part * cut, cut)],
            lambda o, part=part: share.at[o, pl.ds(part * cut, cut)],
            order,
        )
        for part, order in ((0, forth), (1, back))
    ]
    halo_number = 4
    down_number = 6

    ep_next = lax.rem(me_ep + 1, n_ep)
    barrier = pltpu.get_barrier_semaphore()
    greeted = [{"ep": partner_of(me_ep, offset, n_ep)} for offset in range(1, n_ep)]
    greeted += [{"tp": flipped(me_tp, bit)} for bit in tp_order]
    for where in greeted:
        pl.semaphore_signal(barrier, inc=1, device_id=where, device_id_type=MESH)
    take_input = [
        local_copy(moe_input_out, tokens.at[pl.ds(0, moe_input_out.shape[0])]),
        local_copy(in_gain_out, in_gain),
    ]
    take_router = [
        local_copy(group_router_out, group_router),
        local_copy(expert_router_out, expert_router),
        local_copy(routes_out, routes),
    ]
    take_rows = [
        local_copy(keys, key_rows.at[pl.ds(WINDOW, group_rows)]),
        local_copy(values, value_rows.at[pl.ds(WINDOW, group_rows)]),
        local_copy(queries_out, queries),
    ]
    take_gate = local_copy(gate_weight, gates.at[0])
    take_up = local_copy(up_weight, ups.at[0])
    take_down = local_copy(down_weight, downs.at[0])
    own_columns = pl.ds(pl.multiple_of(me_ep * columns, columns), columns)
    take_share = local_copy(out_weight.at[:, own_columns], share.at[0, pl.ds(0, out_weight.shape[0])])
    pl.semaphore_wait(barrier, len(greeted))

    core = lax.rem(me_tp, 2)

    def start_by_core(copies):
        @pl.when(core == 0)
        def _():
            for copy in copies:
                copy.start()

        @pl.when(core == 1)
        def _():
            for copy in copies[::-1]:
                copy.start()

    for step in range(len(forth)):
        gate_spread.first(step)
        up_spread.first(step)
        if step == 0:
            halo = []
            last_rows = pl.ds(group_rows - WINDOW, WINDOW)
            for place, (source, target) in enumerate(((keys, key_rows), (values, value_rows))):
                halo.append(
                    send(
                        source.at[last_rows],
                        target.at[pl.ds(0, WINDOW)],
                        ep_send.at[halo_number + place, 0],
                        ep_recv.at[halo_number + place, 0],
                        {"ep": ep_next},
                    )
                )

    for copy in take_input:
        copy.wait()
    normed = scale_rows(tokens[pl.ds(0, rows)].astype(F32), in_gain[...]).astype(BF16)
    tokens[pl.ds(0, rows)] = normed
    for copy in take_router:
        copy.wait()

    def logits_of(router):
        return lax.dot_general(
            router[...], normed, (((1,), (1,)), ((), ())), preferred_element_type=F32
        )

    group_logits, expert_logits = logits_of(group_router), logits_of(expert_router)
    experts, groups = expert_logits.shape[0], group_logits.shape[0]
    per_group = experts // groups
    group_shifted = jnp.exp(group_logits - jnp.max(group_logits, axis=0, keepdims=True))
    group_prob = group_shifted / jnp.sum(group_shifted, axis=0, keepdims=True)
    expert_ids = lax.broadcasted_iota(jnp.int32, (experts, rows), 0)
    visited = [routes[k : k + 1] for k in range(routes.shape[0])]
    matches = [expert_ids == visit for visit in visited]
    picked = [
        jnp.sum(jnp.where(match, expert_logits, 0.0), axis=0, keepdims=True) for match in matches
    ]
    highest = functools.reduce(jnp.maximum, picked)
    picked = [jnp.exp(p - highest) for p in picked]
    picked_sum = functools.reduce(jnp.add, picked)
    table = jnp.zeros((experts, rows), F32)
    for visit, match, p in zip(visited, matches, picked):
        chosen = jnp.zeros((1, rows), F32)
        for g in range(groups):
            inside = (visit >= g * per_group) & (visit < (g + 1) * per_group)
            chosen = chosen + jnp.where(inside, group_prob[g : g + 1], 0.0)
        table = table + jnp.where(match, chosen * (p / picked_sum), 0.0)
    tables[0] = jnp.zeros(tables.shape[1:], F32)
    tables[0, pl.ds(0, experts)] = table

    coming = {}
    steps = len(tp_order)

    def span_of(position):
        return pl.ds(position * rows, rows)

    def token_send(position, step, started=True):
        target = position + (1 << step)
        where = {"tp": flipped(me_tp, tp_order[step])}
        coming[target] = [
            send(
                source.at[at],
                source.at[to],
                tp_send.at[number, target],
                tp_recv.at[number, target],
                where,
                started,
            )
            for number, source, at, to in (
                (1, tables, position, target),
                (0, tokens, span_of(position), span_of(target)),
            )
        ]
        return coming[target]

    def token_wait(position):
        if position:
            for copy in coming[position]:
                copy.wait_recv()

    token_send(0, steps - 1)
    start_by_core([copy for step in range(steps - 1) for copy in token_send(0, step, False)])

    def to_all(number, source_of, target_of):
        waits = []
        for position in range(1, n_tp):
            other = partner_of(me_tp, tp_offsets[position], n_tp)
            waits.append(
                send(
                    source_of(other),
                    target_of(position),
                    tp_send.at[number, position],
                    tp_recv.at[number, position],
                    {"tp": other},
                )
            )
        return waits

    for copy in take_rows:
        copy.wait()
    for copy in halo:
        copy.wait_recv()
    local_heads = slopes.shape[0]
    per_kv = HEADS // KV_HEADS

    def attend_block(block, carry):
        start = pl.multiple_of(block * WINDOW, WINDOW)
        q = queries[pl.ds(start, WINDOW)]
        k = key_rows[pl.ds(start, 2 * WINDOW)]
        v = value_rows[pl.ds(start, 2 * WINDOW)]
        query_index = lax.broadcasted_iota(jnp.int32, (WINDOW, 2 * WINDOW), 0)
        key_index = lax.broadcasted_iota(jnp.int32, (WINDOW, 2 * WINDOW), 1)
        distance = query_index + WINDOW - key_index
        position = me_ep * group_rows + start + key_index - WINDOW
        valid = (distance >= 0) & (distance < WINDOW) & (position >= 0)
        far = distance.astype(F32)
        outs = []
        for h in range(local_heads):
            kv = (me_tp * local_heads + h) // per_kv
            own = q[:, h * HD : (h + 1) * HD]
            nothing = jnp.zeros_like(own)
            spread = jnp.concatenate(
                [jnp.where(kv == i, own, nothing) for i in range(KV_HEADS)], axis=1
            )
            scores = lax.dot_general(
                spread, k, (((1,), (1,)), ((), ())), preferred_element_type=F32
            ) * (1.0 / math.sqrt(HD))
            scores = jnp.where(valid, scores - slopes[h] * far, -jnp.inf)
            top = jnp.maximum(jnp.max(scores, axis=-1, keepdims=True), sinks[h])
            weights = jnp.exp(scores - top)
            denom = jnp.sum(weights, axis=-1, keepdims=True) + jnp.exp(sinks[h] - top)
            probs = (weights / denom).astype(BF16)
            mixed = jnp.dot(probs, v, preferred_element_type=F32)
            outs.append(
                sum(
                    jnp.where(kv == i, mixed[:, i * HD : (i + 1) * HD], 0.0)
                    for i in range(KV_HEADS)
                )
            )
        joined = outs[0] if local_heads == 1 else jnp.concatenate(outs, axis=1)
        queries[pl.ds(start, WINDOW)] = joined.astype(BF16)
        return carry

    lax.fori_loop(0, group_rows // WINDOW, attend_block, 0)

    def attended_of(index):
        return pl.ds(pl.multiple_of(index * rows, rows), rows)

    pieces[0] = queries[attended_of(me_tp)]

    gate_spread.forward()
    up_spread.forward()

    down_waits = {}
    for c in range(CHUNKS):
        span = pl.ds(c * chunk, chunk)
        for offset in range(1, n_ep):
            down_waits[c, offset] = send(
                down_weight.at[:, span],
                downs.at[offset, :, span],
                ep_send.at[down_number + c, offset],
                ep_recv.at[down_number + c, offset],
                {"ep": partner_of(me_ep, offset, n_ep)},
            )
    for step in range(1, steps):
        for position in range(1, 1 << step):
            token_wait(position)
            token_send(position, step)

    take_gate.wait()
    take_up.wait()

    def hidden_part(offset, inner, first, count):
        span = pl.ds(first * rows, count * rows)
        weight = jnp.concatenate([gates[offset, inner], ups[offset, inner]], axis=1)
        both = jnp.dot(tokens[span], weight, preferred_element_type=F32)
        gated, upped = both[:, :units], both[:, units:]
        expert = partner_of(me_ep, offset, n_ep) * local + inner
        amounts = []
        for position in range(first, first + count):
            block = tables[position]
            expert_row = lax.broadcasted_iota(jnp.int32, block.shape, 0)
            line = jnp.sum(jnp.where(expert_row == expert, block, 0.0), axis=0, keepdims=True)
            amounts.append(jnp.broadcast_to(line, (rows, rows)).T)
        amount = jnp.concatenate(amounts, axis=0)[:, :units]
        product = gated / (1.0 + jnp.exp(-gated)) * upped * amount
        product = jnp.where(amount > 0, product, 0.0).astype(BF16)
        place = (offset * local + inner) * units
        hidden[span, place : place + units] = product

    side = n_tp // 2
    early = n_tp // 4 + 1
    ranges = [(0, early), (side, early), (early, side - early), (side + early, side - early)]

    def hidden_parts(offset, wanted):
        gate_spread.wait(offset)
        up_spread.wait(offset)
        for first, count in wanted:
            for position in range(first, first + count):
                token_wait(position)
            for inner in range(local):
                hidden_part(offset, inner, first, count)

    for offset in range(n_ep - 1):
        hidden_parts(offset, ranges[:2])
    for offset in range(n_ep - 1):
        hidden_parts(offset, ranges[2:])
    piece_waits = to_all(
        2, lambda other: queries.at[attended_of(other)], lambda position: pieces.at[position]
    )
    take_share.wait()
    share_rows = out_weight.shape[0]
    share_waits = {}

    def share_send(position, step, started=True):
        target = position + (1 << step)
        share_waits[target] = send(
            share.at[0, pl.ds(position * share_rows, share_rows)],
            share.at[0, pl.ds(target * share_rows, share_rows)],
            tp_send.at[3, target],
            tp_recv.at[3, target],
            {"tp": flipped(me_tp, tp_order[step])},
            started,
        )
        return share_waits[target]

    def share_wait(position):
        if position:
            share_waits[position].wait_recv()

    start_by_core([share_send(0, step, False) for step in range(steps - 1)])
    hidden_parts(n_ep - 1, [(0, side), (side, side)])

    take_down.wait()
    rs_order = tp_order[::-1]
    arrivals = {}
    for position in coming:
        for copy in coming[position]:
            copy.wait_send()

    def columns_of(c):
        return pl.ds(c * chunk, chunk)

    def down_of(c):
        return jnp.concatenate(
            [
                downs[offset, inner, c * chunk : (c + 1) * chunk]
                for offset in range(n_ep)
                for inner in range(local)
            ],
            axis=1,
        )

    def down_dot(c, first, count):
        return lax.dot_general(
            hidden[pl.ds(first * rows, count * rows)],
            down_of(c),
            (((1,), (1,)), ((), ())),
            preferred_element_type=F32,
        )

    def reduce_send(c, step, started=True):
        count = n_tp >> (step + 1)
        arrivals[c, step] = send(
            tokens.at[pl.ds(count * rows, count * rows), columns_of(c)],
            landed.at[pl.ds((count - 1) * rows, count * rows), columns_of(c)],
            rs_send.at[c, step],
            rs_recv.at[c, step],
            {"tp": flipped(me_tp, rs_order[step])},
            started,
        )
        return arrivals[c, step]

    def arrived(c, step):
        count = n_tp >> (step + 1)
        arrivals[c, step].wait_recv()
        return landed[pl.ds((count - 1) * rows, count * rows), columns_of(c)].astype(F32)

    def keep(c, value, count):
        upper = count // 2
        tokens[pl.ds(upper * rows, upper * rows), columns_of(c)] = value[upper * rows :].astype(BF16)
        held[pl.ds(0, upper * rows), columns_of(c)] = value[: upper * rows]

    def reduce_open(c):
        for offset in range(1, n_ep):
            down_waits[c, offset].wait_recv()
        tokens[pl.ds(side * rows, side * rows), columns_of(c)] = down_dot(c, side, side).astype(BF16)
        reduce_send(c, 0)
        return down_dot(c, 0, side)

    def reduce_kept(c, step):
        count = n_tp >> (step + 1)
        return held[pl.ds(0, count * rows), columns_of(c)] + arrived(c, step)

    crossed = {}

    def share_across(offset):
        for spread in share_spreads:
            spread.wait(offset)
        crossed[offset] = send(
            share.at[offset, pl.ds(0, 2 * cut)],
            share.at[offset, pl.ds(2 * cut, 2 * cut)],
            tp_send.at[4, offset],
            tp_recv.at[4, offset],
            {"tp": flipped(me_tp, 1)},
        )

    def project(offset):
        if offset not in crossed:
            share_across(offset)
        crossed[offset].wait_recv()
        joined = jnp.concatenate([pieces[position] for position in range(n_tp)], axis=1)
        place = pl.multiple_of(partner_of(me_ep, offset, n_ep) * columns, columns)
        projected[:, pl.ds(place, columns)] = jnp.dot(
            joined, share[offset], preferred_element_type=F32
        )

    for tick in range(CHUNKS + LAG * (steps - 1)):
        leaving = []
        if tick < CHUNKS:
            value = reduce_open(tick)
            keep(tick, value + arrived(tick, 0), side)
            leaving.append(reduce_send(tick, 1, False))
        for step in range(1, steps - 1):
            c = tick - LAG * step
            if 0 <= c < CHUNKS:
                keep(c, reduce_kept(c, step), n_tp >> (step + 1))
                leaving.append(reduce_send(c, step + 1, False))
        if leaving:
            start_by_core(leaving)
        c = tick - LAG * (steps - 1)
        if c >= 0:
            total[:, columns_of(c)] = reduce_kept(c, steps - 1)
        if tick == 0:
            for step in range(1, steps - 1):
                for position in range(1, 1 << step):
                    share_wait(position)
                    share_send(position, step)
        if tick == SHARE_FIRST:
            for position in range(1, side):
                share_wait(position)
            share_across(0)
            for step in range(len(forth)):
                for spread in share_spreads:
                    spread.first(step)
        if tick == SHARE_ON:
            for spread in share_spreads:
                spread.forward()
            for offset in forth:
                share_across(offset)
            for copy in piece_waits:
                copy.wait_recv()
            project(0)

    for offset in range(1, n_ep):
        if offset not in crossed:
            share_across(offset)
    for offset in range(1, n_ep):
        project(offset)
    for copy in sent:
        copy.wait_send()


def finish(projected, total, mix_gain, out_gain, mixer_output, moe_output):
    mixer_output[...] = scale_rows(projected[...], mix_gain[...]).astype(BF16)
    moe_output[...] = scale_rows(total[...], out_gain[...]).astype(BF16)


def per_device(n_ep, n_tp, *arguments):
    (queries, keys, values, slopes, sinks, out_weight, mix_gain, moe_input, in_gain, out_gain) = (
        arguments[:10]
    )
    group_router, expert_router, routes, gate_weight, up_weight, down_weight = arguments[10:]
    rows, width = moe_input.shape
    group_rows = rows * n_tp
    local, _, units = gate_weight.shape
    columns = width // n_ep
    experts, groups = expert_router.shape[1], group_router.shape[1]
    whole = pl.BlockSpec(memory_space=pltpu.VMEM)
    scalar = pl.BlockSpec(memory_space=pltpu.SMEM)
    outside = pl.BlockSpec(memory_space=pl.ANY)
    steps = (n_tp - 1).bit_length()
    copies = 6 + CHUNKS
    projected, total = pl.pallas_call(
        functools.partial(kernel, n_ep, n_tp),
        out_shape=[jax.ShapeDtypeStruct((rows, width), F32)] * 2,
        in_specs=[outside] * 3 + [scalar] * 2 + [outside] * 9,
        out_specs=[whole, whole],
        scratch_shapes=[
            pltpu.VMEM(queries.shape, BF16),
            pltpu.VMEM((1, width), F32),
            pltpu.VMEM((groups, width), BF16),
            pltpu.VMEM((experts, width), BF16),
            pltpu.VMEM((routes.shape[1], rows), jnp.int32),
            pltpu.VMEM((n_ep, local, width, units), BF16),
            pltpu.VMEM((n_ep, local, width, units), BF16),
            pltpu.VMEM((n_ep, local, width, units), BF16),
            pltpu.VMEM((group_rows, width), BF16),
            pltpu.VMEM((n_tp, max(8, experts), rows), F32),
            pltpu.VMEM((WINDOW + group_rows, keys.shape[1]), BF16),
            pltpu.VMEM((WINDOW + group_rows, values.shape[1]), BF16),
            pltpu.VMEM((n_tp, rows, queries.shape[1]), BF16),
            pltpu.VMEM((n_ep, out_weight.shape[0] * n_tp, columns), BF16),
            pltpu.VMEM((group_rows, n_ep * local * units), BF16),
            pltpu.VMEM((group_rows - rows, width), BF16),
            pltpu.VMEM((group_rows // 4, width), F32),
            pltpu.SemaphoreType.DMA((16,)),
            pltpu.SemaphoreType.DMA((copies, n_ep)),
            pltpu.SemaphoreType.DMA((copies, n_ep)),
            pltpu.SemaphoreType.DMA((5, max(n_tp, n_ep))),
            pltpu.SemaphoreType.DMA((5, max(n_tp, n_ep))),
            pltpu.SemaphoreType.DMA((CHUNKS, steps)),
            pltpu.SemaphoreType.DMA((CHUNKS, steps)),
        ],
        compiler_params=pltpu.CompilerParams(
            collective_id=0, has_side_effects=True, vmem_limit_bytes=67000000
        ),
    )(
        queries,
        keys,
        values,
        slopes,
        sinks,
        out_weight,
        moe_input,
        in_gain[None],
        group_router.T,
        expert_router.T,
        routes.T,
        gate_weight,
        up_weight,
        down_weight,
    )
    return pl.pallas_call(
        finish,
        out_shape=[jax.ShapeDtypeStruct((rows, width), BF16)] * 2,
        in_specs=[whole] * 4,
        out_specs=[whole] * 2,
    )(projected, total, mix_gain[None], out_gain[None])


def solution(mesh):
    return jax.shard_map(
        functools.partial(per_device, mesh.shape["ep"], mesh.shape["tp"]),
        mesh=mesh,
        in_specs=(
            P("ep", "tp"),
            P("ep", None),
            P("ep", None),
            P("tp"),
            P("tp"),
            P("tp", None),
            P(),
            P(("ep", "tp"), None),
            P(),
            P(),
            P(),
            P(),
            P(("ep", "tp"), None),
            P("ep", None, "tp"),
            P("ep", None, "tp"),
            P("ep", None, "tp"),
        ),
        out_specs=(P(("ep", "tp"), None), P(("ep", "tp"), None)),
        check_vma=False,
    )
```

```python
import functools
import math

import jax
import jax.numpy as jnp
from jax import lax
from jax.experimental import pallas as pl
from jax.experimental.pallas import tpu as pltpu
from jax.sharding import PartitionSpec as P

HEADS = 16
HD = 64
KV_HEADS = 4
WINDOW = 128
CHUNKS = 8
LAG = 2


eps = 1e-06
MESH = pl.DeviceIdType.MESH
F32 = jnp.float32
BF16 = jnp.bfloat16


def flipped(index, bit):
    return index + bit - 2 * bit * ((index // bit) % 2)


def partner_of(index, offset, size):
    bit = 1
    while bit < size:
        if offset & bit:
            index = flipped(index, bit)
        bit *= 2
    return index


def bits_of(size):
    return [1 << i for i in range((size - 1).bit_length())]


def scale_rows(matrix, gain):
    mean_square = jnp.mean(matrix * matrix, axis=-1, keepdims=True)
    return matrix * lax.rsqrt(mean_square + eps) * gain


def kernel(
    n_ep,
    n_tp,
    queries_out,
    keys,
    values,
    slopes,
    sinks,
    out_weight,
    moe_input_out,
    in_gain_out,
    mix_gain_out,
    group_router_out,
    expert_router_out,
    routes_out,
    gate_weight,
    up_weight,
    down_weight,
    mixed,
    total,
    queries,
    in_gain,
    mix_gain,
    group_router,
    expert_router,
    routes,
    gates,
    ups,
    downs,
    tokens,
    tables,
    key_rows,
    value_rows,
    pieces,
    share,
    projected,
    hidden,
    landed,
    passing,
    local_sem,
    ep_send,
    ep_recv,
    tp_send,
    tp_recv,
    core_send,
    core_recv,
    all_send,
    all_recv,
    rs_send,
    rs_recv,
):
    me_ep, me_tp = lax.axis_index("ep"), lax.axis_index("tp")
    rows, width = moe_input_out.shape
    local, _, units = gate_weight.shape
    group_rows = rows * n_tp
    columns = width // n_ep
    chunk = width // CHUNKS
    own_span = pl.ds(pl.multiple_of(lax.axis_index("tp") // 2 * rows, rows), rows)
    forth = bits_of(n_ep)
    back = forth[::-1]
    chips = n_tp // 2
    chip, core = me_tp // 2, lax.rem(me_tp, 2)
    sibling = {"tp": flipped(me_tp, 1)}
    flows = (
        (1, {"tp": me_tp + 2}, chips - 1 - chip, chip),
        (-1, {"tp": me_tp - 2}, chip, chips - 1 - chip),
    )
    cut = share.shape[1] // 4

    sent = []
    locals_ = []

    class Tracked:
        def __init__(self, copy):
            self.copy, self.gone, self.here = copy, False, False

        def start(self):
            self.copy.start()

        def wait_send(self):
            if not self.gone:
                self.copy.wait_send()
                self.gone = True

        def wait_recv(self):
            if not self.here:
                self.copy.wait_recv()
                self.here = True

    def local_copy(source, target):
        copy = pltpu.make_async_copy(source, target, local_sem.at[len(locals_)])
        copy.start()
        locals_.append(copy)
        return copy

    def send(source, target, send_sem, recv_sem, where, started=True):
        copy = pltpu.make_async_remote_copy(
            src_ref=source,
            dst_ref=target,
            send_sem=send_sem,
            recv_sem=recv_sem,
            device_id=where,
            device_id_type=MESH,
        )
        if started:
            copy.start()
        sent.append(Tracked(copy))
        return sent[-1]

    class Spread:
        def __init__(self, number, own, slot_of, order):
            self.number, self.own, self.slot_of, self.order = number, own, slot_of, order
            self.coming = {}

        def post(self, source, offset, bit):
            target = offset ^ bit
            self.coming[target] = send(
                source,
                self.slot_of(target),
                ep_send.at[self.number, target],
                ep_recv.at[self.number, target],
                {"ep": flipped(me_ep, bit)},
            )

        def first(self, step):
            self.post(self.own, 0, self.order[step])

        def wait(self, offset):
            if offset:
                self.coming[offset].wait_recv()

        def forward(self):
            held = [0]
            for bit in self.order:
                for offset in held:
                    if offset:
                        self.wait(offset)
                        self.post(self.slot_of(offset), offset, bit)
                held = held + [offset ^ bit for offset in held]

    gate_spread = Spread(0, gate_weight, lambda o: gates.at[o], forth)
    up_spread = Spread(1, up_weight, lambda o: ups.at[o], back)
    share_spreads = [
        Spread(
            2 + part,
            share.at[0, pl.ds(part * cut, cut)],
            lambda o, part=part: share.at[o, pl.ds(part * cut, cut)],
            order,
        )
        for part, order in ((0, forth), (1, back))
    ]
    halo_number = 4
    down_number = 6

    ep_next = lax.rem(me_ep + 1, n_ep)
    barrier = pltpu.get_barrier_semaphore()
    greeted = [{"ep": partner_of(me_ep, offset, n_ep)} for offset in range(1, n_ep)]
    greeted += [sibling]
    for where in greeted:
        pl.semaphore_signal(barrier, inc=1, device_id=where, device_id_type=MESH)
    for _, following, ahead, _ in flows:

        @pl.when(ahead > 0)
        def _(following=following):
            pl.semaphore_signal(barrier, inc=1, device_id=following, device_id_type=MESH)

    take_input = [
        local_copy(moe_input_out, tokens.at[own_span]),
        local_copy(in_gain_out, in_gain),
    ]
    take_router = [
        local_copy(group_router_out, group_router),
        local_copy(expert_router_out, expert_router),
        local_copy(routes_out, routes),
    ]
    take_rows = [
        local_copy(keys, key_rows.at[pl.ds(WINDOW, group_rows)]),
        local_copy(values, value_rows.at[pl.ds(WINDOW, group_rows)]),
        local_copy(queries_out, queries),
    ]
    take_mix = local_copy(mix_gain_out, mix_gain)
    take_gate = local_copy(gate_weight, gates.at[0])
    take_up = local_copy(up_weight, ups.at[0])
    take_down = local_copy(down_weight, downs.at[0])
    own_columns = pl.ds(pl.multiple_of(me_ep * columns, columns), columns)
    take_share = local_copy(
        out_weight.at[:, own_columns],
        share.at[
            0,
            pl.ds(
                pl.multiple_of(me_tp // 2 * out_weight.shape[0], out_weight.shape[0]),
                out_weight.shape[0],
            ),
        ],
    )
    neighbours = sum(jnp.where(ahead > 0, 1, 0) for _, _, ahead, _ in flows)
    pl.semaphore_wait(barrier, len(greeted) + neighbours)

    halo = []
    last_rows = pl.ds(group_rows - WINDOW, WINDOW)
    for place, (source, target) in enumerate(((keys, key_rows), (values, value_rows))):
        halo.append(
            send(
                source.at[last_rows],
                target.at[pl.ds(0, WINDOW)],
                ep_send.at[halo_number + place, 0],
                ep_recv.at[halo_number + place, 0],
                {"ep": ep_next},
            )
        )
    for step in range(len(forth)):
        gate_spread.first(step)
        up_spread.first(step)

    for copy in take_input:
        copy.wait()
    normed = scale_rows(tokens[own_span].astype(F32), in_gain[...]).astype(BF16)
    tokens[own_span] = normed
    for copy in take_router:
        copy.wait()

    def logits_of(router):
        return lax.dot_general(
            router[...], normed, (((1,), (1,)), ((), ())), preferred_element_type=F32
        )

    group_logits, expert_logits = logits_of(group_router), logits_of(expert_router)
    experts, groups = expert_logits.shape[0], group_logits.shape[0]
    per_group = experts // groups
    group_shifted = jnp.exp(group_logits - jnp.max(group_logits, axis=0, keepdims=True))
    group_prob = group_shifted / jnp.sum(group_shifted, axis=0, keepdims=True)
    expert_ids = lax.broadcasted_iota(jnp.int32, (experts, rows), 0)
    visited = [routes[k : k + 1] for k in range(routes.shape[0])]
    matches = [expert_ids == visit for visit in visited]
    picked = [
        jnp.sum(jnp.where(match, expert_logits, 0.0), axis=0, keepdims=True) for match in matches
    ]
    highest = functools.reduce(jnp.maximum, picked)
    picked = [jnp.exp(p - highest) for p in picked]
    picked_sum = functools.reduce(jnp.add, picked)
    table = jnp.zeros((experts, rows), F32)
    for visit, match, p in zip(visited, matches, picked):
        chosen = jnp.zeros((1, rows), F32)
        for g in range(groups):
            inside = (visit >= g * per_group) & (visit < (g + 1) * per_group)
            chosen = chosen + jnp.where(inside, group_prob[g : g + 1], 0.0)
        table = table + jnp.where(match, chosen * (p / picked_sum), 0.0)
    height = tables.shape[0] // n_tp
    if height > experts:
        table = jnp.concatenate([table, jnp.zeros((height - experts, rows), F32)], axis=0)
    tables[pl.ds(pl.multiple_of(chip * height, height), height)] = table

    def span_of(block):
        return pl.ds(pl.multiple_of(block * rows, rows), rows)

    class Line:
        def __init__(self, number, ref, part=0, parts=1):
            self.number, self.ref = number, ref
            self.height = ref.shape[0] // n_tp // parts
            self.part, self.parts = part, parts

        def at(self, block):
            start = (block * self.parts + self.part) * self.height
            return self.ref.at[pl.ds(pl.multiple_of(start, self.height), self.height)]

        def copy(self, flow, far, block, where):
            number = 2 * self.number + flow
            return pltpu.make_async_remote_copy(
                src_ref=self.at(block),
                dst_ref=self.at(block),
                send_sem=tp_send.at[number, far],
                recv_sem=tp_recv.at[number, far],
                device_id=where,
                device_id_type=MESH,
            )

        def push(self, far, act="start"):
            for flow, (way, following, ahead, behind) in enumerate(flows):

                @pl.when((ahead > 0) & (behind >= far - 1))
                def _(flow=flow, way=way, following=following):
                    getattr(self.copy(flow, far, chip - way * (far - 1), following), act)()

        def take(self, far):
            for flow, (way, following, ahead, behind) in enumerate(flows):

                @pl.when(behind >= far)
                def _(flow=flow, way=way):
                    self.copy(flow, far, chip - way * far, sibling).wait_recv()

    class Across:
        def __init__(self, line):
            self.line = line

        def copy(self, flow, far, block):
            number = 2 * self.line.number + flow
            return pltpu.make_async_remote_copy(
                src_ref=self.line.at(block),
                dst_ref=self.line.at(chips + block),
                send_sem=core_send.at[number, far],
                recv_sem=core_recv.at[number, far],
                device_id=sibling,
                device_id_type=MESH,
            )

        def act(self, far, what):
            if far == 0:
                getattr(self.copy(0, 0, chip), what)()
                return
            for flow, (way, _, _, behind) in enumerate(flows):

                @pl.when(behind >= far)
                def _(flow=flow, way=way):
                    getattr(self.copy(flow, far, chip - way * far), what)()

    token_lines = [Line(0, tables), Line(1, tokens, 0, 2), Line(2, tokens, 1, 2)]
    token_across = [Across(line) for line in token_lines]

    def tokens_on(far):
        for line in token_lines:
            if far:
                line.take(far)
            if far + 1 < chips:
                line.push(far + 1)
        for line in token_across:
            line.act(far, "start")

    def tokens_across(far):
        for line in token_across:
            line.act(far, "wait_recv")

    tokens_on(0)

    def to_all(number, source_of, target_of):
        waits = []
        for offset in range(1, n_tp):
            other = partner_of(me_tp, offset, n_tp)
            waits.append(
                send(
                    source_of(other),
                    target_of(offset % 2 * chips + chip),
                    all_send.at[number, offset],
                    all_recv.at[number, offset],
                    {"tp": other},
                    False,
                )
            )
        return waits

    def start_pieces(inner):
        for offset, copy in zip(range(1, n_tp), piece_waits):
            place = partner_of(me_tp, offset, n_tp) // 2
            inside = (place > 0) & (place < chips - 1)

            @pl.when(inside if inner else jnp.logical_not(inside))
            def _(copy=copy):
                copy.start()

    for copy in take_rows:
        copy.wait()
    for copy in halo:
        copy.wait_recv()
    local_heads = slopes.shape[0]
    per_kv = HEADS // KV_HEADS

    def attend_block(block, carry):
        start = pl.multiple_of(block * WINDOW, WINDOW)
        q = queries[pl.ds(start, WINDOW)]
        k = key_rows[pl.ds(start, 2 * WINDOW)]
        v = value_rows[pl.ds(start, 2 * WINDOW)]
        query_index = lax.broadcasted_iota(jnp.int32, (WINDOW, 2 * WINDOW), 0)
        key_index = lax.broadcasted_iota(jnp.int32, (WINDOW, 2 * WINDOW), 1)
        distance = query_index + WINDOW - key_index
        position = me_ep * group_rows + start + key_index - WINDOW
        valid = (distance >= 0) & (distance < WINDOW) & (position >= 0)
        far = distance.astype(F32)
        outs = []
        for h in range(local_heads):
            kv = (me_tp * local_heads + h) // per_kv
            own = q[:, h * HD : (h + 1) * HD]
            nothing = jnp.zeros_like(own)
            spread = jnp.concatenate(
                [jnp.where(kv == i, own, nothing) for i in range(KV_HEADS)], axis=1
            )
            scores = lax.dot_general(
                spread, k, (((1,), (1,)), ((), ())), preferred_element_type=F32
            ) * (1.0 / math.sqrt(HD))
            scores = jnp.where(valid, scores - slopes[h] * far, -jnp.inf)
            top = jnp.maximum(jnp.max(scores, axis=-1, keepdims=True), sinks[h])
            weights = jnp.exp(scores - top)
            denom = jnp.sum(weights, axis=-1, keepdims=True) + jnp.exp(sinks[h] - top)
            probs = (weights / denom).astype(BF16)
            mixed = jnp.dot(probs, v, preferred_element_type=F32)
            outs.append(
                sum(
                    jnp.where(kv == i, mixed[:, i * HD : (i + 1) * HD], 0.0)
                    for i in range(KV_HEADS)
                )
            )
        joined = outs[0] if local_heads == 1 else jnp.concatenate(outs, axis=1)
        queries[pl.ds(start, WINDOW)] = joined.astype(BF16)
        return carry

    lax.fori_loop(0, group_rows // WINDOW, attend_block, 0)

    def attended_of(index):
        return pl.ds(pl.multiple_of(index * rows, rows), rows)

    pieces[chip] = queries[attended_of(me_tp)]

    gate_spread.forward()
    up_spread.forward()

    down_waits = {}
    for c in range(CHUNKS):
        span = pl.ds(c * chunk, chunk)
        for offset in range(1, n_ep):
            down_waits[c, offset] = send(
                down_weight.at[:, span],
                downs.at[offset, :, span],
                ep_send.at[down_number + c, offset],
                ep_recv.at[down_number + c, offset],
                {"ep": partner_of(me_ep, offset, n_ep)},
            )
    for far in range(1, chips - 1):
        tokens_on(far)
    take_share.wait()
    share_line = Line(3, share.at[0])
    share_line.push(1)

    take_gate.wait()
    take_up.wait()

    def hidden_part(offset, inner, first, count):
        span = pl.ds(pl.multiple_of(first * rows, rows), count * rows)
        weight = jnp.concatenate([gates[offset, inner], ups[offset, inner]], axis=1)
        both = jnp.dot(tokens[span], weight, preferred_element_type=F32)
        gated, upped = both[:, :units], both[:, units:]
        expert = partner_of(me_ep, offset, n_ep) * local + inner
        amounts = []
        height = tables.shape[0] // n_tp
        for number in range(count):
            block = tables[pl.ds(pl.multiple_of((first + number) * height, height), height)]
            expert_row = lax.broadcasted_iota(jnp.int32, block.shape, 0)
            line = jnp.sum(jnp.where(expert_row == expert, block, 0.0), axis=0, keepdims=True)
            amounts.append(jnp.broadcast_to(line, (rows, rows)).T)
        amount = jnp.concatenate(amounts, axis=0)[:, :units]
        product = gated / (1.0 + jnp.exp(-gated)) * upped * amount
        product = jnp.where(amount > 0, product, 0.0).astype(BF16)
        place = (offset * local + inner) * units
        hidden[span, place : place + units] = product

    def sweep(wanted, offsets):
        def block_step(block, carry):
            far = jnp.abs(lax.rem(block, chips) - chip)

            @pl.when(wanted(far))
            def _():
                for offset in offsets:
                    for inner in range(local):
                        hidden_part(offset, inner, block, 1)

            return carry

        lax.fori_loop(0, n_tp, block_step, 0)

    for offset in range(n_ep - 1):
        gate_spread.wait(offset)
        up_spread.wait(offset)
    for far in range(chips - 1):
        tokens_across(far)
    piece_waits = to_all(
        0, lambda other: queries.at[attended_of(other)], lambda place: pieces.at[place]
    )
    start_pieces(True)
    sweep(lambda far: far < chips - 1, range(n_ep - 1))
    tokens_on(chips - 1)
    gate_spread.wait(n_ep - 1)
    up_spread.wait(n_ep - 1)
    sweep(lambda far: far < chips - 1, [n_ep - 1])
    tokens_across(chips - 1)
    sweep(lambda far: far == chips - 1, range(n_ep))

    take_down.wait()
    arrivals = {}
    for line in token_lines:
        for far in range(1, chips):
            line.push(far, "wait_send")
    for line in token_across:
        for far in range(chips):
            line.act(far, "wait_send")

    def columns_of(c):
        return pl.ds(pl.multiple_of(c * chunk, chunk), chunk)

    def down_of(c):
        return jnp.concatenate(
            [
                downs[offset, inner, c * chunk : (c + 1) * chunk]
                for offset in range(n_ep)
                for inner in range(local)
            ],
            axis=1,
        )

    def down_dot(c, first, count):
        return lax.dot_general(
            hidden[pl.ds(first * rows, count * rows)],
            down_of(c),
            (((1,), (1,)), ((), ())),
            preferred_element_type=F32,
        )

    def reduce_open(c):
        for offset in range(1, n_ep):
            down_waits[c, offset].wait_recv()
        upper = pl.ds(chips * rows, chips * rows)
        tokens[upper, columns_of(c)] = down_dot(c, chips, chips).astype(BF16)
        arrivals[c] = send(
            tokens.at[upper, columns_of(c)],
            landed.at[:, columns_of(c)],
            rs_send.at[2 * CHUNKS + c, 0],
            rs_recv.at[2 * CHUNKS + c, 0],
            sibling,
        )

    def reduce_pair(c):
        lower = pl.ds(0, chips * rows)
        value = down_dot(c, 0, chips)
        arrivals[c].wait_recv()
        value = value + landed[:, columns_of(c)].astype(F32)
        tokens[lower, columns_of(c)] = value.astype(BF16)
        total[:, columns_of(c)] = sum(
            jnp.where(chip == b, value[b * rows : (b + 1) * rows], 0.0) for b in range(chips)
        )

    def passed(flow, c, far, block, place):
        return pltpu.make_async_remote_copy(
            src_ref=tokens.at[span_of(block), columns_of(c)],
            dst_ref=passing.at[span_of(place), columns_of(c)],
            send_sem=rs_send.at[flow * CHUNKS + c, far],
            recv_sem=rs_recv.at[flow * CHUNKS + c, far],
            device_id=flows[flow][1],
            device_id_type=MESH,
        )

    def place_of(flow, far, block):
        return jnp.where(far == 1, chips, block) if flow else block

    def reduce_flow(flow, c):
        way, _, ahead, behind = flows[flow]
        going = (c >= 0) & (c < CHUNKS)
        for far in range(chips - 1, 0, -1):
            block = chip + way * far
            source = (span_of(block), columns_of(c))

            if far + 1 < chips:

                @pl.when(going & (ahead >= far) & (behind > 0))
                def _():
                    passed(flow, c, far + 1, chip, block).wait_recv()
                    tokens[source] = (
                        tokens[source].astype(F32) + passing[source].astype(F32)
                    ).astype(BF16)

            @pl.when(going & (ahead >= far))
            def _():
                passed(flow, c, far, block, place_of(flow, far, block)).start()

        @pl.when(going & (behind > 0))
        def _():
            place = place_of(flow, 1, chip)
            passed(flow, c, 1, chip, place).wait_recv()
            columns_here = columns_of(c)
            total[:, columns_here] += passing[span_of(place), columns_here].astype(F32)

    def reduce_gone(c, carry):
        for flow, (way, _, ahead, _) in enumerate(flows):
            for far in range(1, chips):

                @pl.when(ahead >= far)
                def _(flow=flow, far=far, way=way):
                    block = chip + way * far
                    passed(flow, c, far, block, block).wait_send()

        return carry

    crossed = {}

    def share_across(offset):
        for spread in share_spreads:
            spread.wait(offset)
        crossed[offset] = send(
            share.at[offset, pl.ds(0, 2 * cut)],
            share.at[offset, pl.ds(2 * cut, 2 * cut)],
            all_send.at[1, offset],
            all_recv.at[1, offset],
            {"tp": flipped(me_tp, 1)},
        )

    def project(offset):
        if offset not in crossed:
            share_across(offset)
        crossed[offset].wait_recv()
        joined = jnp.concatenate([pieces[position] for position in range(n_tp)], axis=1)
        place = pl.multiple_of(partner_of(me_ep, offset, n_ep) * columns, columns)
        projected[:, pl.ds(place, columns)] = jnp.dot(
            joined, share[offset], preferred_element_type=F32
        )

    reduce_open(0)
    for tick in range(CHUNKS + LAG * (chips - 1)):
        if tick + 1 < CHUNKS:
            reduce_open(tick + 1)
        if tick < CHUNKS:
            reduce_pair(tick)
        for flow, (_, _, _, behind) in enumerate(flows):
            reduce_flow(flow, tick - LAG * behind)
        if tick == 0:
            start_pieces(False)
        if 0 < tick < chips:
            share_line.take(tick)
            if tick + 1 < chips:
                share_line.push(tick + 1)
        if tick == chips - 1:
            share_across(0)
            for step in range(len(forth)):
                for spread in share_spreads:
                    spread.first(step)
        if tick == chips + 2:
            for spread in share_spreads:
                spread.forward()
            for offset in forth:
                share_across(offset)
            for copy in piece_waits:
                copy.wait_recv()
            project(0)
        if tick == max(CHUNKS, chips) + 3:
            for offset in range(1, n_ep):
                if offset not in crossed:
                    share_across(offset)
            for offset in range(1, n_ep):
                project(offset)
            take_mix.wait()
            mixed[...] = scale_rows(projected[...], mix_gain[...]).astype(BF16)

    for far in range(1, chips):
        share_line.push(far, "wait_send")
    lax.fori_loop(0, CHUNKS, reduce_gone, 0)
    for copy in sent:
        copy.wait_send()


def finish(mixed, total, out_gain, mixer_output, moe_output):
    mixer_output[...] = mixed[...]
    moe_output[...] = scale_rows(total[...], out_gain[...]).astype(BF16)


def per_device(n_ep, n_tp, *arguments):
    (queries, keys, values, slopes, sinks, out_weight, mix_gain, moe_input, in_gain, out_gain) = (
        arguments[:10]
    )
    group_router, expert_router, routes, gate_weight, up_weight, down_weight = arguments[10:]
    rows, width = moe_input.shape
    group_rows = rows * n_tp
    local, _, units = gate_weight.shape
    columns = width // n_ep
    experts, groups = expert_router.shape[1], group_router.shape[1]
    whole = pl.BlockSpec(memory_space=pltpu.VMEM)
    scalar = pl.BlockSpec(memory_space=pltpu.SMEM)
    outside = pl.BlockSpec(memory_space=pl.ANY)
    chips = n_tp // 2
    copies = 6 + CHUNKS
    mixed, total = pl.pallas_call(
        functools.partial(kernel, n_ep, n_tp),
        out_shape=[jax.ShapeDtypeStruct((rows, width), kind) for kind in (BF16, F32)],
        in_specs=[outside] * 3 + [scalar] * 2 + [outside] * 10,
        out_specs=[whole, whole],
        scratch_shapes=[
            pltpu.VMEM(queries.shape, BF16),
            pltpu.VMEM((1, width), F32),
            pltpu.VMEM((1, width), F32),
            pltpu.VMEM((groups, width), BF16),
            pltpu.VMEM((experts, width), BF16),
            pltpu.VMEM((routes.shape[1], rows), jnp.int32),
            pltpu.VMEM((n_ep, local, width, units), BF16),
            pltpu.VMEM((n_ep, local, width, units), BF16),
            pltpu.VMEM((n_ep, local, width, units), BF16),
            pltpu.VMEM((group_rows, width), BF16),
            pltpu.VMEM((n_tp * max(8, experts), rows), F32),
            pltpu.VMEM((WINDOW + group_rows, keys.shape[1]), BF16),
            pltpu.VMEM((WINDOW + group_rows, values.shape[1]), BF16),
            pltpu.VMEM((n_tp, rows, queries.shape[1]), BF16),
            pltpu.VMEM((n_ep, out_weight.shape[0] * n_tp, columns), BF16),
            pltpu.VMEM((rows, width), F32),
            pltpu.VMEM((group_rows, n_ep * local * units), BF16),
            pltpu.VMEM((chips * rows, width), BF16),
            pltpu.VMEM((chips * rows + rows, width), BF16),
            pltpu.SemaphoreType.DMA((16,)),
            pltpu.SemaphoreType.DMA((copies, n_ep)),
            pltpu.SemaphoreType.DMA((copies, n_ep)),
            pltpu.SemaphoreType.DMA((8, chips)),
            pltpu.SemaphoreType.DMA((8, chips)),
            pltpu.SemaphoreType.DMA((6, chips)),
            pltpu.SemaphoreType.DMA((6, chips)),
            pltpu.SemaphoreType.DMA((2, max(n_tp, n_ep))),
            pltpu.SemaphoreType.DMA((2, max(n_tp, n_ep))),
            pltpu.SemaphoreType.DMA((3 * CHUNKS, chips)),
            pltpu.SemaphoreType.DMA((3 * CHUNKS, chips)),
        ],
        compiler_params=pltpu.CompilerParams(
            collective_id=0, has_side_effects=True, vmem_limit_bytes=67000000
        ),
    )(
        queries,
        keys,
        values,
        slopes,
        sinks,
        out_weight,
        moe_input,
        in_gain[None],
        mix_gain[None],
        group_router.T,
        expert_router.T,
        routes.T,
        gate_weight,
        up_weight,
        down_weight,
    )
    return pl.pallas_call(
        finish,
        out_shape=[jax.ShapeDtypeStruct((rows, width), BF16)] * 2,
        in_specs=[whole] * 3,
        out_specs=[whole] * 2,
    )(mixed, total, out_gain[None])


def solution(mesh):
    return jax.shard_map(
        functools.partial(per_device, mesh.shape["ep"], mesh.shape["tp"]),
        mesh=mesh,
        in_specs=(
            P("ep", "tp"),
            P("ep", None),
            P("ep", None),
            P("tp"),
            P("tp"),
            P("tp", None),
            P(),
            P(("ep", "tp"), None),
            P(),
            P(),
            P(),
            P(),
            P(("ep", "tp"), None),
            P("ep", None, "tp"),
            P("ep", None, "tp"),
            P("ep", None, "tp"),
        ),
        out_specs=(P(("ep", "tp"), None), P(("ep", "tp"), None)),
        check_vma=False,
    )
```

```python
import functools
import math

import jax
import jax.numpy as jnp
from jax import lax
from jax.experimental import pallas as pl
from jax.experimental.pallas import tpu as pltpu
from jax.sharding import PartitionSpec as P

HEADS = 16
HD = 64
KV_HEADS = 4
WINDOW = 128
CHUNKS = 8
LAG = 2


eps = 1e-06
MESH = pl.DeviceIdType.MESH
F32 = jnp.float32
BF16 = jnp.bfloat16


def flipped(index, bit):
    return index + bit - 2 * bit * ((index // bit) % 2)


def partner_of(index, offset, size):
    bit = 1
    while bit < size:
        if offset & bit:
            index = flipped(index, bit)
        bit *= 2
    return index


def bits_of(size):
    return [1 << i for i in range((size - 1).bit_length())]


def scale_rows(matrix, gain):
    mean_square = jnp.mean(matrix * matrix, axis=-1, keepdims=True)
    return matrix * lax.rsqrt(mean_square + eps) * gain


def kernel(
    n_ep,
    n_tp,
    queries_out,
    keys,
    values,
    slopes,
    sinks,
    out_weight,
    moe_input_out,
    in_gain_out,
    mix_gain_out,
    group_router_out,
    expert_router_out,
    routes_out,
    gate_weight,
    up_weight,
    down_weight,
    mixed,
    total,
    queries,
    in_gain,
    mix_gain,
    group_router,
    expert_router,
    routes,
    gates,
    ups,
    downs,
    tokens,
    tables,
    key_rows,
    value_rows,
    pieces,
    share,
    projected,
    hidden,
    landed,
    passing,
    local_sem,
    ep_send,
    ep_recv,
    tp_send,
    tp_recv,
    core_send,
    core_recv,
    all_send,
    all_recv,
    rs_send,
    rs_recv,
):
    me_ep, me_tp = lax.axis_index("ep"), lax.axis_index("tp")
    rows, width = moe_input_out.shape
    local, _, units = gate_weight.shape
    group_rows = rows * n_tp
    columns = width // n_ep
    chunk = width // CHUNKS
    own_span = pl.ds(pl.multiple_of(lax.axis_index("tp") // 2 * rows, rows), rows)
    forth = bits_of(n_ep)
    back = forth[::-1]
    chips = n_tp // 2
    chip, core = me_tp // 2, lax.rem(me_tp, 2)
    sibling = {"tp": flipped(me_tp, 1)}
    flows = (
        (1, {"tp": me_tp + 2}, chips - 1 - chip, chip),
        (-1, {"tp": me_tp - 2}, chip, chips - 1 - chip),
    )
    cut = share.shape[1] // 4

    sent = []
    locals_ = []

    class Tracked:
        def __init__(self, copy):
            self.copy, self.gone, self.here = copy, False, False

        def start(self):
            self.copy.start()

        def wait_send(self):
            if not self.gone:
                self.copy.wait_send()
                self.gone = True

        def wait_recv(self):
            if not self.here:
                self.copy.wait_recv()
                self.here = True

    def local_copy(source, target):
        copy = pltpu.make_async_copy(source, target, local_sem.at[len(locals_)])
        copy.start()
        locals_.append(copy)
        return copy

    def send(source, target, send_sem, recv_sem, where, started=True):
        copy = pltpu.make_async_remote_copy(
            src_ref=source,
            dst_ref=target,
            send_sem=send_sem,
            recv_sem=recv_sem,
            device_id=where,
            device_id_type=MESH,
        )
        if started:
            copy.start()
        sent.append(Tracked(copy))
        return sent[-1]

    class Spread:
        def __init__(self, number, own, slot_of, order):
            self.number, self.own, self.slot_of, self.order = number, own, slot_of, order
            self.coming = {}

        def post(self, source, offset, bit):
            target = offset ^ bit
            self.coming[target] = send(
                source,
                self.slot_of(target),
                ep_send.at[self.number, target],
                ep_recv.at[self.number, target],
                {"ep": flipped(me_ep, bit)},
            )

        def first(self, step):
            self.post(self.own, 0, self.order[step])

        def wait(self, offset):
            if offset:
                self.coming[offset].wait_recv()

        def forward(self):
            held = [0]
            for bit in self.order:
                for offset in held:
                    if offset:
                        self.wait(offset)
                        self.post(self.slot_of(offset), offset, bit)
                held = held + [offset ^ bit for offset in held]

    gate_spread = Spread(0, gate_weight, lambda o: gates.at[o], forth)
    up_spread = Spread(1, up_weight, lambda o: ups.at[o], back)
    share_spreads = [
        Spread(
            2 + part,
            share.at[0, pl.ds(part * cut, cut)],
            lambda o, part=part: share.at[o, pl.ds(part * cut, cut)],
            order,
        )
        for part, order in ((0, forth), (1, back))
    ]
    halo_number = 4
    down_number = 6

    ep_next = lax.rem(me_ep + 1, n_ep)
    barrier = pltpu.get_barrier_semaphore()
    greeted = [{"ep": partner_of(me_ep, offset, n_ep)} for offset in range(1, n_ep)]
    greeted += [sibling]
    for where in greeted:
        pl.semaphore_signal(barrier, inc=1, device_id=where, device_id_type=MESH)
    for _, following, ahead, _ in flows:

        @pl.when(ahead > 0)
        def _(following=following):
            pl.semaphore_signal(barrier, inc=1, device_id=following, device_id_type=MESH)

    take_input = [
        local_copy(moe_input_out, tokens.at[own_span]),
        local_copy(in_gain_out, in_gain),
    ]
    take_router = [
        local_copy(group_router_out, group_router),
        local_copy(expert_router_out, expert_router),
        local_copy(routes_out, routes),
    ]
    take_rows = [
        local_copy(keys, key_rows.at[pl.ds(WINDOW, group_rows)]),
        local_copy(values, value_rows.at[pl.ds(WINDOW, group_rows)]),
        local_copy(queries_out, queries),
    ]
    take_mix = local_copy(mix_gain_out, mix_gain)
    take_gate = local_copy(gate_weight, gates.at[0])
    take_up = local_copy(up_weight, ups.at[0])
    take_down = local_copy(down_weight, downs.at[0])
    own_columns = pl.ds(pl.multiple_of(me_ep * columns, columns), columns)
    take_share = local_copy(
        out_weight.at[:, own_columns],
        share.at[
            0,
            pl.ds(
                pl.multiple_of(me_tp // 2 * out_weight.shape[0], out_weight.shape[0]),
                out_weight.shape[0],
            ),
        ],
    )
    for copy in take_input:
        copy.wait()
    normed = scale_rows(tokens[own_span].astype(F32), in_gain[...]).astype(BF16)
    tokens[own_span] = normed
    neighbours = sum(jnp.where(ahead > 0, 1, 0) for _, _, ahead, _ in flows)
    pl.semaphore_wait(barrier, len(greeted) + neighbours)

    halo = []
    last_rows = pl.ds(group_rows - WINDOW, WINDOW)
    for place, (source, target) in enumerate(((keys, key_rows), (values, value_rows))):
        halo.append(
            send(
                source.at[last_rows],
                target.at[pl.ds(0, WINDOW)],
                ep_send.at[halo_number + place, 0],
                ep_recv.at[halo_number + place, 0],
                {"ep": ep_next},
            )
        )
    for step in range(len(forth)):
        gate_spread.first(step)
        up_spread.first(step)

    def span_of(block):
        return pl.ds(pl.multiple_of(block * rows, rows), rows)

    class Line:
        def __init__(self, number, ref, part=0, parts=1):
            self.number, self.ref = number, ref
            self.height = ref.shape[0] // n_tp // parts
            self.part, self.parts = part, parts

        def at(self, block):
            start = (block * self.parts + self.part) * self.height
            return self.ref.at[pl.ds(pl.multiple_of(start, self.height), self.height)]

        def copy(self, flow, far, block, where):
            number = 2 * self.number + flow
            return pltpu.make_async_remote_copy(
                src_ref=self.at(block),
                dst_ref=self.at(block),
                send_sem=tp_send.at[number, far],
                recv_sem=tp_recv.at[number, far],
                device_id=where,
                device_id_type=MESH,
            )

        def push(self, far, act="start"):
            for flow, (way, following, ahead, behind) in enumerate(flows):

                @pl.when((ahead > 0) & (behind >= far - 1))
                def _(flow=flow, way=way, following=following):
                    getattr(self.copy(flow, far, chip - way * (far - 1), following), act)()

        def take(self, far):
            for flow, (way, following, ahead, behind) in enumerate(flows):

                @pl.when(behind >= far)
                def _(flow=flow, way=way):
                    self.copy(flow, far, chip - way * far, sibling).wait_recv()

    class Across:
        def __init__(self, line):
            self.line = line

        def copy(self, flow, far, block):
            number = 2 * self.line.number + flow
            return pltpu.make_async_remote_copy(
                src_ref=self.line.at(block),
                dst_ref=self.line.at(chips + block),
                send_sem=core_send.at[number, far],
                recv_sem=core_recv.at[number, far],
                device_id=sibling,
                device_id_type=MESH,
            )

        def act(self, far, what):
            if far == 0:
                getattr(self.copy(0, 0, chip), what)()
                return
            for flow, (way, _, _, behind) in enumerate(flows):

                @pl.when(behind >= far)
                def _(flow=flow, way=way):
                    getattr(self.copy(flow, far, chip - way * far), what)()

    token_lines = [Line(0, tables), Line(1, tokens, 0, 2), Line(2, tokens, 1, 2)]
    token_across = [Across(line) for line in token_lines]

    def tokens_on(far, chosen=slice(None)):
        for line in token_lines[chosen]:
            if far:
                line.take(far)
            if far + 1 < chips:
                line.push(far + 1)
        for line in token_across[chosen]:
            line.act(far, "start")

    def tokens_across(far):
        for line in token_across:
            line.act(far, "wait_recv")

    tokens_on(0, slice(1, None))
    for copy in take_router:
        copy.wait()

    def logits_of(router):
        return lax.dot_general(
            router[...], normed, (((1,), (1,)), ((), ())), preferred_element_type=F32
        )

    group_logits, expert_logits = logits_of(group_router), logits_of(expert_router)
    experts, groups = expert_logits.shape[0], group_logits.shape[0]
    per_group = experts // groups
    group_shifted = jnp.exp(group_logits - jnp.max(group_logits, axis=0, keepdims=True))
    group_prob = group_shifted / jnp.sum(group_shifted, axis=0, keepdims=True)
    expert_ids = lax.broadcasted_iota(jnp.int32, (experts, rows), 0)
    visited = [routes[k : k + 1] for k in range(routes.shape[0])]
    matches = [expert_ids == visit for visit in visited]
    picked = [
        jnp.sum(jnp.where(match, expert_logits, 0.0), axis=0, keepdims=True) for match in matches
    ]
    highest = functools.reduce(jnp.maximum, picked)
    picked = [jnp.exp(p - highest) for p in picked]
    picked_sum = functools.reduce(jnp.add, picked)
    table = jnp.zeros((experts, rows), F32)
    for visit, match, p in zip(visited, matches, picked):
        chosen = jnp.zeros((1, rows), F32)
        for g in range(groups):
            inside = (visit >= g * per_group) & (visit < (g + 1) * per_group)
            chosen = chosen + jnp.where(inside, group_prob[g : g + 1], 0.0)
        table = table + jnp.where(match, chosen * (p / picked_sum), 0.0)
    height = tables.shape[0] // n_tp
    if height > experts:
        table = jnp.concatenate([table, jnp.zeros((height - experts, rows), F32)], axis=0)
    tables[pl.ds(pl.multiple_of(chip * height, height), height)] = table

    tokens_on(0, slice(0, 1))

    def to_all(number, source_of, target_of):
        waits = []
        for offset in range(1, n_tp):
            other = partner_of(me_tp, offset, n_tp)
            waits.append(
                send(
                    source_of(other),
                    target_of(offset % 2 * chips + chip),
                    all_send.at[number, offset],
                    all_recv.at[number, offset],
                    {"tp": other},
                    False,
                )
            )
        return waits

    def start_pieces(inner):
        for offset, copy in zip(range(1, n_tp), piece_waits):
            place = partner_of(me_tp, offset, n_tp) // 2
            inside = (place > 0) & (place < chips - 1)

            @pl.when(inside if inner else jnp.logical_not(inside))
            def _(copy=copy):
                copy.start()

    for copy in take_rows:
        copy.wait()
    for copy in halo:
        copy.wait_recv()
    local_heads = slopes.shape[0]
    per_kv = HEADS // KV_HEADS

    def attend_block(block, carry):
        start = pl.multiple_of(block * WINDOW, WINDOW)
        q = queries[pl.ds(start, WINDOW)]
        k = key_rows[pl.ds(start, 2 * WINDOW)]
        v = value_rows[pl.ds(start, 2 * WINDOW)]
        query_index = lax.broadcasted_iota(jnp.int32, (WINDOW, 2 * WINDOW), 0)
        key_index = lax.broadcasted_iota(jnp.int32, (WINDOW, 2 * WINDOW), 1)
        distance = query_index + WINDOW - key_index
        position = me_ep * group_rows + start + key_index - WINDOW
        valid = (distance >= 0) & (distance < WINDOW) & (position >= 0)
        far = distance.astype(F32)
        outs = []
        for h in range(local_heads):
            kv = (me_tp * local_heads + h) // per_kv
            own = q[:, h * HD : (h + 1) * HD]
            nothing = jnp.zeros_like(own)
            spread = jnp.concatenate(
                [jnp.where(kv == i, own, nothing) for i in range(KV_HEADS)], axis=1
            )
            scores = lax.dot_general(
                spread, k, (((1,), (1,)), ((), ())), preferred_element_type=F32
            ) * (1.0 / math.sqrt(HD))
            scores = jnp.where(valid, scores - slopes[h] * far, -jnp.inf)
            top = jnp.maximum(jnp.max(scores, axis=-1, keepdims=True), sinks[h])
            weights = jnp.exp(scores - top)
            denom = jnp.sum(weights, axis=-1, keepdims=True) + jnp.exp(sinks[h] - top)
            probs = (weights / denom).astype(BF16)
            mixed = jnp.dot(probs, v, preferred_element_type=F32)
            outs.append(
                sum(
                    jnp.where(kv == i, mixed[:, i * HD : (i + 1) * HD], 0.0)
                    for i in range(KV_HEADS)
                )
            )
        joined = outs[0] if local_heads == 1 else jnp.concatenate(outs, axis=1)
        queries[pl.ds(start, WINDOW)] = joined.astype(BF16)
        return carry

    lax.fori_loop(0, group_rows // WINDOW, attend_block, 0)

    def attended_of(index):
        return pl.ds(pl.multiple_of(index * rows, rows), rows)

    pieces[chip] = queries[attended_of(me_tp)]

    gate_spread.forward()
    up_spread.forward()

    down_waits = {}
    for c in range(CHUNKS):
        span = pl.ds(c * chunk, chunk)
        for offset in range(1, n_ep):
            down_waits[c, offset] = send(
                down_weight.at[:, span],
                downs.at[offset, :, span],
                ep_send.at[down_number + c, offset],
                ep_recv.at[down_number + c, offset],
                {"ep": partner_of(me_ep, offset, n_ep)},
            )
    for far in range(1, chips - 1):
        tokens_on(far)
    take_share.wait()
    share_line = Line(3, share.at[0])
    share_line.push(1)

    take_gate.wait()
    take_up.wait()

    def hidden_part(offset, inner, first, count):
        span = pl.ds(pl.multiple_of(first * rows, rows), count * rows)
        weight = jnp.concatenate([gates[offset, inner], ups[offset, inner]], axis=1)
        both = jnp.dot(tokens[span], weight, preferred_element_type=F32)
        gated, upped = both[:, :units], both[:, units:]
        expert = partner_of(me_ep, offset, n_ep) * local + inner
        amounts = []
        height = tables.shape[0] // n_tp
        for number in range(count):
            block = tables[pl.ds(pl.multiple_of((first + number) * height, height), height)]
            expert_row = lax.broadcasted_iota(jnp.int32, block.shape, 0)
            line = jnp.sum(jnp.where(expert_row == expert, block, 0.0), axis=0, keepdims=True)
            amounts.append(jnp.broadcast_to(line, (rows, rows)).T)
        amount = jnp.concatenate(amounts, axis=0)[:, :units]
        product = gated / (1.0 + jnp.exp(-gated)) * upped * amount
        product = jnp.where(amount > 0, product, 0.0).astype(BF16)
        place = (offset * local + inner) * units
        hidden[span, place : place + units] = product

    def sweep(wanted, offsets):
        def block_step(block, carry):
            far = jnp.abs(lax.rem(block, chips) - chip)

            @pl.when(wanted(far))
            def _():
                for offset in offsets:
                    for inner in range(local):
                        hidden_part(offset, inner, block, 1)

            return carry

        lax.fori_loop(0, n_tp, block_step, 0)

    for offset in range(n_ep - 1):
        gate_spread.wait(offset)
        up_spread.wait(offset)
    for far in range(chips - 1):
        tokens_across(far)
    piece_waits = to_all(
        0, lambda other: queries.at[attended_of(other)], lambda place: pieces.at[place]
    )
    start_pieces(True)
    sweep(lambda far: far < chips - 1, range(n_ep - 1))
    tokens_on(chips - 1)
    gate_spread.wait(n_ep - 1)
    up_spread.wait(n_ep - 1)
    sweep(lambda far: far < chips - 1, [n_ep - 1])
    tokens_across(chips - 1)
    sweep(lambda far: far == chips - 1, range(n_ep))

    take_down.wait()
    arrivals = {}
    for line in token_lines:
        for far in range(1, chips):
            line.push(far, "wait_send")
    for line in token_across:
        for far in range(chips):
            line.act(far, "wait_send")

    def columns_of(c):
        return pl.ds(pl.multiple_of(c * chunk, chunk), chunk)

    def down_of(c):
        return jnp.concatenate(
            [
                downs[offset, inner, c * chunk : (c + 1) * chunk]
                for offset in range(n_ep)
                for inner in range(local)
            ],
            axis=1,
        )

    def down_dot(c, first, count):
        return lax.dot_general(
            hidden[pl.ds(first * rows, count * rows)],
            down_of(c),
            (((1,), (1,)), ((), ())),
            preferred_element_type=F32,
        )

    def reduce_open(c):
        for offset in range(1, n_ep):
            down_waits[c, offset].wait_recv()
        upper = pl.ds(chips * rows, chips * rows)
        tokens[upper, columns_of(c)] = down_dot(c, chips, chips).astype(BF16)
        arrivals[c] = send(
            tokens.at[upper, columns_of(c)],
            landed.at[:, columns_of(c)],
            rs_send.at[2 * CHUNKS + c, 0],
            rs_recv.at[2 * CHUNKS + c, 0],
            sibling,
        )

    def reduce_pair(c):
        lower = pl.ds(0, chips * rows)
        value = down_dot(c, 0, chips)
        arrivals[c].wait_recv()
        value = value + landed[:, columns_of(c)].astype(F32)
        tokens[lower, columns_of(c)] = value.astype(BF16)
        total[:, columns_of(c)] = sum(
            jnp.where(chip == b, value[b * rows : (b + 1) * rows], 0.0) for b in range(chips)
        )

    def passed(flow, c, far, block, place):
        return pltpu.make_async_remote_copy(
            src_ref=tokens.at[span_of(block), columns_of(c)],
            dst_ref=passing.at[span_of(place), columns_of(c)],
            send_sem=rs_send.at[flow * CHUNKS + c, far],
            recv_sem=rs_recv.at[flow * CHUNKS + c, far],
            device_id=flows[flow][1],
            device_id_type=MESH,
        )

    def place_of(flow, far, block):
        return jnp.where(far == 1, chips, block) if flow else block

    def reduce_flow(flow, c):
        way, _, ahead, behind = flows[flow]
        going = (c >= 0) & (c < CHUNKS)
        for far in range(chips - 1, 0, -1):
            block = chip + way * far
            source = (span_of(block), columns_of(c))

            if far + 1 < chips:

                @pl.when(going & (ahead >= far) & (behind > 0))
                def _():
                    passed(flow, c, far + 1, chip, block).wait_recv()
                    tokens[source] = (
                        tokens[source].astype(F32) + passing[source].astype(F32)
                    ).astype(BF16)

            @pl.when(going & (ahead >= far))
            def _():
                passed(flow, c, far, block, place_of(flow, far, block)).start()

        @pl.when(going & (behind > 0))
        def _():
            place = place_of(flow, 1, chip)
            passed(flow, c, 1, chip, place).wait_recv()
            columns_here = columns_of(c)
            total[:, columns_here] += passing[span_of(place), columns_here].astype(F32)

    def reduce_gone(c, carry):
        for flow, (way, _, ahead, _) in enumerate(flows):
            for far in range(1, chips):

                @pl.when(ahead >= far)
                def _(flow=flow, far=far, way=way):
                    block = chip + way * far
                    passed(flow, c, far, block, block).wait_send()

        return carry

    crossed = {}

    def share_across(offset):
        for spread in share_spreads:
            spread.wait(offset)
        crossed[offset] = send(
            share.at[offset, pl.ds(0, 2 * cut)],
            share.at[offset, pl.ds(2 * cut, 2 * cut)],
            all_send.at[1, offset],
            all_recv.at[1, offset],
            {"tp": flipped(me_tp, 1)},
        )

    def project(offset):
        if offset not in crossed:
            share_across(offset)
        crossed[offset].wait_recv()
        joined = jnp.concatenate([pieces[position] for position in range(n_tp)], axis=1)
        place = pl.multiple_of(partner_of(me_ep, offset, n_ep) * columns, columns)
        projected[:, pl.ds(place, columns)] = jnp.dot(
            joined, share[offset], preferred_element_type=F32
        )

    reduce_open(0)
    for tick in range(CHUNKS + LAG * (chips - 1)):
        if tick + 1 < CHUNKS:
            reduce_open(tick + 1)
        if tick < CHUNKS:
            reduce_pair(tick)
        for flow, (_, _, _, behind) in enumerate(flows):
            reduce_flow(flow, tick - LAG * behind)
        if tick == 0:
            start_pieces(False)
        if 0 < tick < chips:
            share_line.take(tick)
            if tick + 1 < chips:
                share_line.push(tick + 1)
        if tick == chips - 1:
            share_across(0)
            for step in range(len(forth)):
                for spread in share_spreads:
                    spread.first(step)
        if tick == chips + 2:
            for spread in share_spreads:
                spread.forward()
            for offset in forth:
                share_across(offset)
            for copy in piece_waits:
                copy.wait_recv()
            project(0)
        if tick == max(CHUNKS, chips) + 3:
            for offset in range(1, n_ep):
                if offset not in crossed:
                    share_across(offset)
            for offset in range(1, n_ep):
                project(offset)
            take_mix.wait()
            mixed[...] = scale_rows(projected[...], mix_gain[...]).astype(BF16)

    for far in range(1, chips):
        share_line.push(far, "wait_send")
    lax.fori_loop(0, CHUNKS, reduce_gone, 0)
    for copy in sent:
        copy.wait_send()


def finish(mixed, total, out_gain, mixer_output, moe_output):
    mixer_output[...] = mixed[...]
    moe_output[...] = scale_rows(total[...], out_gain[...]).astype(BF16)


def per_device(n_ep, n_tp, *arguments):
    (queries, keys, values, slopes, sinks, out_weight, mix_gain, moe_input, in_gain, out_gain) = (
        arguments[:10]
    )
    group_router, expert_router, routes, gate_weight, up_weight, down_weight = arguments[10:]
    rows, width = moe_input.shape
    group_rows = rows * n_tp
    local, _, units = gate_weight.shape
    columns = width // n_ep
    experts, groups = expert_router.shape[1], group_router.shape[1]
    whole = pl.BlockSpec(memory_space=pltpu.VMEM)
    scalar = pl.BlockSpec(memory_space=pltpu.SMEM)
    outside = pl.BlockSpec(memory_space=pl.ANY)
    chips = n_tp // 2
    copies = 6 + CHUNKS
    mixed, total = pl.pallas_call(
        functools.partial(kernel, n_ep, n_tp),
        out_shape=[jax.ShapeDtypeStruct((rows, width), kind) for kind in (BF16, F32)],
        in_specs=[outside] * 3 + [scalar] * 2 + [outside] * 10,
        out_specs=[whole, whole],
        scratch_shapes=[
            pltpu.VMEM(queries.shape, BF16),
            pltpu.VMEM((1, width), F32),
            pltpu.VMEM((1, width), F32),
            pltpu.VMEM((groups, width), BF16),
            pltpu.VMEM((experts, width), BF16),
            pltpu.VMEM((routes.shape[1], rows), jnp.int32),
            pltpu.VMEM((n_ep, local, width, units), BF16),
            pltpu.VMEM((n_ep, local, width, units), BF16),
            pltpu.VMEM((n_ep, local, width, units), BF16),
            pltpu.VMEM((group_rows, width), BF16),
            pltpu.VMEM((n_tp * max(8, experts), rows), F32),
            pltpu.VMEM((WINDOW + group_rows, keys.shape[1]), BF16),
            pltpu.VMEM((WINDOW + group_rows, values.shape[1]), BF16),
            pltpu.VMEM((n_tp, rows, queries.shape[1]), BF16),
            pltpu.VMEM((n_ep, out_weight.shape[0] * n_tp, columns), BF16),
            pltpu.VMEM((rows, width), F32),
            pltpu.VMEM((group_rows, n_ep * local * units), BF16),
            pltpu.VMEM((chips * rows, width), BF16),
            pltpu.VMEM((chips * rows + rows, width), BF16),
            pltpu.SemaphoreType.DMA((16,)),
            pltpu.SemaphoreType.DMA((copies, n_ep)),
            pltpu.SemaphoreType.DMA((copies, n_ep)),
            pltpu.SemaphoreType.DMA((8, chips)),
            pltpu.SemaphoreType.DMA((8, chips)),
            pltpu.SemaphoreType.DMA((6, chips)),
            pltpu.SemaphoreType.DMA((6, chips)),
            pltpu.SemaphoreType.DMA((2, max(n_tp, n_ep))),
            pltpu.SemaphoreType.DMA((2, max(n_tp, n_ep))),
            pltpu.SemaphoreType.DMA((3 * CHUNKS, chips)),
            pltpu.SemaphoreType.DMA((3 * CHUNKS, chips)),
        ],
        compiler_params=pltpu.CompilerParams(
            collective_id=0, has_side_effects=True, vmem_limit_bytes=67000000
        ),
    )(
        queries,
        keys,
        values,
        slopes,
        sinks,
        out_weight,
        moe_input,
        in_gain[None],
        mix_gain[None],
        group_router.T,
        expert_router.T,
        routes.T,
        gate_weight,
        up_weight,
        down_weight,
    )
    return pl.pallas_call(
        finish,
        out_shape=[jax.ShapeDtypeStruct((rows, width), BF16)] * 2,
        in_specs=[whole] * 3,
        out_specs=[whole] * 2,
    )(mixed, total, out_gain[None])


def solution(mesh):
    return jax.shard_map(
        functools.partial(per_device, mesh.shape["ep"], mesh.shape["tp"]),
        mesh=mesh,
        in_specs=(
            P("ep", "tp"),
            P("ep", None),
            P("ep", None),
            P("tp"),
            P("tp"),
            P("tp", None),
            P(),
            P(("ep", "tp"), None),
            P(),
            P(),
            P(),
            P(),
            P(("ep", "tp"), None),
            P("ep", None, "tp"),
            P("ep", None, "tp"),
            P("ep", None, "tp"),
        ),
        out_specs=(P(("ep", "tp"), None), P(("ep", "tp"), None)),
        check_vma=False,
    )
```
